32 devices in a mesh: rep: 2 (over x), fs: 8 (over z, y), tp: 2 (over core).
Axes of the slice: x: 2, y: 2, z: 4, core: 2. Of those that a mesh axis runs over, the one named last changes fastest.
Arguments:
- resid: bfloat16 [4096, 2048], P(('rep', 'fs'), 'tp'), may hold values from -6 to 6
- norm_gains: float32 [3, 2048], replicated, may hold values from 0.1 to 1.9
- gate_one: bfloat16 [2048, 5632], P('fs', 'tp'), may hold values from -0.125 to 0.125
- up_one: bfloat16 [2048, 5632], P('fs', 'tp'), may hold values from -0.125 to 0.125
- down_one: bfloat16 [5632, 2048], P('tp', 'fs'), may hold values from -0.109375 to 0.109375
- proj_u: bfloat16 [2048, 1024], P('fs', 'tp'), may hold values from -0.125 to 0.125
- proj_v: bfloat16 [2048, 1024], P('fs', 'tp'), may hold values from -0.125 to 0.125
- spatial: bfloat16 [8, 128, 128], P('tp'), may hold values from -0.5 to 0.5
- spatial_bias: float32 [8, 128], P('tp'), may hold values from 0.1 to 1.9
- mix_gain: float32 [1024], P('tp'), may hold values from 0.1 to 1.9
- head_gain: float32 [1024], P('tp'), may hold values from 0.1 to 1.9
- proj_out: bfloat16 [1024, 2048], P('tp', 'fs'), may hold values from -0.25 to 0.25
- gate_two: bfloat16 [2048, 5632], P('fs', 'tp'), may hold values from -0.125 to 0.125
- up_two: bfloat16 [2048, 5632], P('fs', 'tp'), may hold values from -0.125 to 0.125
- down_two: bfloat16 [5632, 2048], P('tp', 'fs'), may hold values from -0.109375 to 0.109375
Outputs:
- layer_out: bfloat16 [4096, 2048], P(('rep', 'fs'), 'tp')
The draws below stay inside these ranges and needn't reach their ends.
All inputs are finite; a program needn't handle non-finite values.
Results may differ from the reference program's by a relative error of at most 0.019.
Values may be sent and summed in bfloat16 or wider, within the bound.
A program may use at most 128 MiB of HBM per device.

```python
import jax
import jax.numpy as jnp
from jax import lax

D = 2048
FF = 5632
HEADS = 8
HEAD_DIM = 128
BLOCK = 128
SPAN = 64
GM = 1024
TOKENS = 4096
N_TP = 2


def raised(entries, stream_key, source, target, shards_of, factor):
    owner, partner = [(jnp.arange(entries.shape[position]) // (entries.shape[position] // shards_of)).reshape([-1 if axis == position else 1 for axis in range(entries.ndim)]) for position in (source, target)]
    chosen = jax.random.permutation(stream_key, shards_of)[partner]
    strong = (owner == chosen) | (owner == (partner + shards_of // 2) % shards_of)
    return jnp.where(strong, factor * entries, entries)


def steps_of(own_key, shape, pieces, low, largest):
    def one(dim, shards_of):
        draws = jax.random.uniform(jax.random.fold_in(jax.random.fold_in(own_key, 6), dim), (shards_of,), jnp.float32, low / len(pieces), largest / len(pieces))
        return jnp.repeat(jnp.exp(draws), shape[dim] // shards_of).reshape((-1,) + (1,) * (len(shape) - dim - 1))

    factor_of = one(*pieces[0])
    for cut in pieces[1:]:
        factor_of = factor_of * one(*cut)
    return factor_of


def centred(rng, shape, deviation, reach, cuts=(), held_as=jnp.bfloat16):
    level = steps_of(rng, shape, cuts, -0.22, 0.18) if cuts else 1.0
    drawn = jax.random.normal(rng, shape, jnp.float32) * deviation * level
    return jnp.minimum(jnp.maximum(drawn, -reach), reach).astype(held_as)


def bell_draw_with(key, extent, deviation, most, shards, heavy, dtype=jnp.bfloat16):
    result = deviation * jax.random.normal(key, extent, jnp.float32)
    if shards:
        result = result * steps_of(key, extent, shards, -0.22, 0.18)
    return jnp.clip(raised(result, jax.random.fold_in(key, 3), *heavy), -most, most).astype(dtype)


def setup_inputs(seed: int = 0) -> dict:
    key_list = jax.random.split(jax.random.key(seed), 16)
    return {
        "resid": centred(key_list[0], (TOKENS, D), 1.0, 6.0, ((0, 16), (1, 2))),
        "norm_gains": jnp.clip(1.0 + 0.18 * jax.random.normal(key_list[1], (3, D), jnp.float32), 0.1, 1.9),
        "gate_one": centred(key_list[2], (D, FF), D ** -0.5, 0.125, ((0, 8), (1, 2))),
        "up_one": centred(key_list[3], (D, FF), D ** -0.5, 0.125, ((0, 8), (1, 2))),
        "down_one": bell_draw_with(key_list[4], (FF, D), FF ** -0.5, 0.109375, ((0, 2), (1, 8)), (0, 1, 8, 2.0)),
        "proj_u": centred(key_list[5], (D, GM), D ** -0.5, 0.125, ((0, 8), (1, 2))),
        "proj_v": centred(key_list[6], (D, GM), D ** -0.5, 0.125, ((0, 8), (1, 2))),
        "spatial": centred(key_list[7], (HEADS, BLOCK, BLOCK), BLOCK ** -0.5, 0.5, ((0, 2),)),
        "spatial_bias": jnp.clip(1.0 + 0.18 * jax.random.normal(key_list[8], (HEADS, BLOCK), jnp.float32), 0.1, 1.9),
        "mix_gain": jnp.clip(1.0 + 0.18 * jax.random.normal(key_list[9], (GM,), jnp.float32), 0.1, 1.9),
        "head_gain": jnp.clip(1.0 + 0.18 * jax.random.normal(key_list[10], (GM,), jnp.float32), 0.1, 1.9),
        "proj_out": bell_draw_with(key_list[11], (GM, D), GM ** -0.5, 0.25, ((0, 2), (1, 8)), (0, 1, 8, 2.0)),
        "gate_two": centred(key_list[12], (D, FF), D ** -0.5, 0.125, ((0, 8), (1, 2))),
        "up_two": centred(key_list[13], (D, FF), D ** -0.5, 0.125, ((0, 8), (1, 2))),
        "down_two": bell_draw_with(key_list[14], (FF, D), FF ** -0.5, 0.109375, ((0, 2), (1, 8)), (0, 1, 8, 2.0)),
    }


def rms_scale(values, gain):
    return values * lax.rsqrt(lax.optimization_barrier(jnp.mean(values * values, axis=-1, keepdims=True)) + 1e-06) * gain

def blockwise_sum(hidden, weight, parts):
    width = hidden.shape[1] // parts
    total = jnp.zeros((hidden.shape[0], weight.shape[1]), jnp.float32)
    for index in range(parts):
        partial_sum = jnp.dot(hidden[:, index * width:(index + 1) * width], weight[index * width:(index + 1) * width], preferred_element_type=jnp.float32)
        rounded = lax.optimization_barrier(partial_sum.astype(jnp.bfloat16))
        total = total + rounded.astype(jnp.float32)
    return total

def feed_forward(stream, gain, gate_weight, up_weight, down_weight):
    normed = rms_scale(stream.astype(jnp.float32), gain).astype(jnp.bfloat16)
    gate = jnp.dot(normed, gate_weight, preferred_element_type=jnp.float32)
    up_part = jnp.dot(normed, up_weight, preferred_element_type=jnp.float32)
    hidden = (jax.nn.silu(gate) * up_part).astype(jnp.bfloat16)
    return blockwise_sum(hidden, down_weight, N_TP)

def reference(resid, norm_gains, gate_one, up_one, down_one, proj_u, proj_v, spatial, spatial_bias, mix_gain, head_gain, proj_out, gate_two, up_two, down_two):
    first = (resid.astype(jnp.float32) + 0.5 * feed_forward(resid, norm_gains[0], gate_one, up_one, down_one)).astype(jnp.bfloat16)
    mnormed = rms_scale(first.astype(jnp.float32), norm_gains[1]).astype(jnp.bfloat16)
    u_part = jnp.dot(mnormed, proj_u, preferred_element_type=jnp.float32)
    v_part = jnp.dot(mnormed, proj_v, preferred_element_type=jnp.float32)
    rows = u_part.shape[0]
    seqs = rows // BLOCK
    gated_u = jax.nn.gelu(u_part).reshape(seqs, BLOCK, HEADS, HEAD_DIM)
    gated_v = jax.nn.gelu(v_part).reshape(seqs, BLOCK, HEADS, HEAD_DIM)
    centre = lax.optimization_barrier(jnp.mean(gated_v, axis=-1, keepdims=True))
    spread = lax.optimization_barrier(jnp.mean(jnp.square(gated_v - centre), axis=-1, keepdims=True))
    vn = ((gated_v - centre) * lax.rsqrt(spread + 1e-05) * mix_gain.reshape(HEADS, HEAD_DIM)).astype(jnp.bfloat16)
    segment = jnp.arange(BLOCK) // SPAN
    causal = segment[:, None] >= segment[None, :]
    masked = jnp.where(causal[None], spatial.astype(jnp.float32), 0.0)
    mixed = jnp.einsum('hts,bshd->bthd', masked, vn.astype(jnp.float32)) + spatial_bias.T[None, :, :, None]
    product = gated_u * mixed
    gated = rms_scale(product, head_gain.reshape(HEADS, HEAD_DIM)).astype(jnp.bfloat16).reshape(rows, HEADS * HEAD_DIM)
    branch = blockwise_sum(gated, proj_out, N_TP)
    second = (first.astype(jnp.float32) + branch).astype(jnp.bfloat16)
    return (second.astype(jnp.float32) + 0.5 * feed_forward(second, norm_gains[2], gate_two, up_two, down_two)).astype(jnp.bfloat16)
```

```python
import functools

import jax
import jax.numpy as jnp
from jax import lax
from jax.experimental import pallas as pl
from jax.experimental.pallas import tpu as pltpu
from jax.sharding import PartitionSpec as P


HEAD_DIM = 128
BLOCK = 128
SPAN = 64


def rms_scale(values, gain):
    return values * lax.rsqrt(jnp.mean(values * values, axis=-1, keepdims=True) + 1e-06) * gain


def normalized(stream, gain):
    whole = lax.all_gather(stream, "tp", axis=1, tiled=True).astype(jnp.float32)
    return rms_scale(whole, gain).astype(jnp.bfloat16)


def accumulate(left, piece):
    return jnp.dot(left, piece, preferred_element_type=jnp.float32)


def folders(normed):

    def single(total, piece, start):
        return accumulate(normed, piece)

    def double(totals, pieces, start):
        return (accumulate(normed, pieces[0]), accumulate(normed, pieces[1]))

    return (single, double)


def ffn_inputs(normed, first_weight, second_weight):
    empty = jnp.zeros((normed.shape[0], first_weight.shape[1]), jnp.float32)
    single, _ = folders(normed)
    result = (
        single(empty, lax.all_gather(first_weight, "fs", axis=0, tiled=True), jnp.int32(0)),
        single(empty, lax.all_gather(second_weight, "fs", axis=0, tiled=True), jnp.int32(0)),
    )
    return result


def mixer_inputs(normed, first_weight, second_weight):
    empty = jnp.zeros((normed.shape[0], first_weight.shape[1]), jnp.float32)
    single, _ = folders(normed)
    result = (
        single(empty, lax.all_gather(first_weight, "fs", axis=0, tiled=True), jnp.int32(0)),
        single(empty, lax.all_gather(second_weight, "fs", axis=0, tiled=True), jnp.int32(0)),
    )
    return result


LANE = 128
MESH = pl.DeviceIdType.MESH
VMEM = pltpu.VMEM


def flip(value, bit):
    return value + bit - 2 * bit * lax.rem(lax.div(value, jnp.int32(bit)), 2)


def xor(value, mask):
    for bit in (1, 2, 4):
        if mask & bit:
            value = flip(value, bit)
    return value


class Place:
    def __init__(self):
        self.rep, self.fs, self.tp = (lax.axis_index(name) for name in ("rep", "fs", "tp"))
        self.y = lax.rem(self.fs, 2)
        self.z = lax.rem(lax.div(self.fs, jnp.int32(2)), 2)
        self.x_peer = {"rep": 1 - self.rep}
        self.y_peer = {"fs": flip(self.fs, 1)}
        self.z_peer = {"fs": flip(self.fs, 2)}
        self.sibling = {"tp": 1 - self.tp}

    def member(self, mask):
        return xor(4 * self.rep + 2 * self.y + self.z, mask)

    def barrier(self):
        semaphore = pltpu.get_barrier_semaphore()
        peers = [{"fs": xor(self.fs, mask)} for mask in range(1, 8)]
        peers += [self.x_peer, self.sibling]
        for peer in peers:
            pl.semaphore_signal(semaphore, inc=1, device_id=peer, device_id_type=MESH)
        pl.semaphore_wait(semaphore, len(peers))


def remote(src, dst, send, recv, peer):
    return pltpu.make_async_remote_copy(
        src_ref=src, dst_ref=dst, send_sem=send, recv_sem=recv,
        device_id=peer, device_id_type=MESH,
    )


def rows_at(index, size):
    return pl.ds(pl.multiple_of(index * size, size), size)


class Shares:
    def __init__(self, units):
        self.tiles = units // LANE // 2
        self.most = -(-self.tiles // 4)
        self.missing = 4 * self.most - self.tiles
        self.base = (self.most - (1 if self.missing else 0)) * LANE
        self.extra = LANE if self.missing else 0
        self.slot = self.most * LANE

    def of(self, place, quarter, core):
        late = 4 - self.missing
        before = jnp.where(
            core == 0, jnp.maximum(quarter - late, 0), jnp.minimum(quarter, self.missing)
        )
        long = jnp.where(core == 0, quarter < late, quarter >= self.missing)
        start = place.rep * self.tiles + quarter * self.most - before
        return start * LANE, long


class Weights:
    def __init__(self, place, shares, shards, whole, sems):
        self.place, self.shares, self.shards, self.whole = place, shares, shards, whole
        self.send_sem, self.recv_sem, self.pass_send, self.pass_recv, self.local = sems
        self.kinds = 6 if shares.extra else 3
        self.quarter = lax.rem(place.fs, 4)

    def source(self, kind, start):
        shares, which = self.shares, kind % 3
        first = start + (shares.base if kind >= 3 else 0)
        size = shares.extra if kind >= 3 else shares.base
        ref = self.shards[which]
        first = jnp.minimum(first, ref.shape[0 if which == 2 else 1] - size)
        cut = pl.ds(pl.multiple_of(first, LANE), size)
        return ref.at[cut, :] if which == 2 else ref.at[:, cut]

    def target(self, kind, owner, core):
        shares, which = self.shares, kind % 3
        first = core * shares.slot + (shares.base if kind >= 3 else 0)
        size = shares.extra if kind >= 3 else shares.base
        cut = pl.ds(pl.multiple_of(first, LANE), size)
        ref = self.whole[which]
        if which == 2:
            return ref.at[cut, rows_at(owner, self.shards[2].shape[1])]
        return ref.at[rows_at(owner, self.shards[which].shape[0]), cut]

    def when(self, kind, long, action):
        if kind >= 3:
            pl.when(long)(action)
        else:
            action()

    def out(self, kind, mask):
        peer = xor(self.place.fs, mask)
        start, long = self.shares.of(self.place, lax.rem(peer, 4), self.place.tp)
        return long, remote(
            self.source(kind, start),
            self.target(kind, self.place.fs, self.place.tp),
            self.send_sem.at[kind, mask],
            self.recv_sem.at[kind, mask],
            {"fs": peer},
        )

    def start(self, pieces):
        for kind, mask in pieces:
            long, copy = self.out(kind, mask)
            self.when(kind, long, copy.start)

    def own(self):
        start, long = self.shares.of(self.place, self.quarter, self.place.tp)
        for kind in range(self.kinds):
            source = self.source(kind, start)
            target = self.target(kind, self.place.fs, self.place.tp)
            here = pltpu.make_async_copy(source, target, self.local.at[kind])
            there = self.passed(kind, 0, source)

            def begin(here=here, there=there):
                here.start()
                there.start()

            self.when(kind, long, begin)

    def passed(self, kind, mask, source=None):
        target = self.target(kind, xor(self.place.fs, mask), self.place.tp)
        return remote(
            target if source is None else source,
            target,
            self.pass_send.at[kind, mask],
            self.pass_recv.at[kind, mask],
            self.place.sibling,
        )

    def blank(self):
        shares = self.shares
        if not shares.extra:
            return
        for core in range(2):
            _, long = shares.of(self.place, self.quarter, core)
            cut = pl.ds(core * shares.slot + shares.base, shares.extra)

            def clear(cut=cut):
                for ref in self.whole[:2]:
                    ref[:, cut] = jnp.zeros((ref.shape[0], shares.extra), ref.dtype)
                down = self.whole[2]
                down[cut, :] = jnp.zeros((shares.extra, down.shape[1]), down.dtype)

            pl.when(jnp.logical_not(long))(clear)

    def forward(self, pieces):
        _, long = self.shares.of(self.place, self.quarter, self.place.tp)
        for kind, mask in pieces:
            def step(kind=kind, mask=mask):
                self.out(kind, mask)[1].wait_recv()
                self.passed(kind, mask).start()

            self.when(kind, long, step)

    def finish(self):
        _, long = self.shares.of(self.place, self.quarter, self.place.tp)
        _, other = self.shares.of(self.place, self.quarter, 1 - self.place.tp)
        start, _ = self.shares.of(self.place, self.quarter, self.place.tp)
        for kind in range(self.kinds):
            here = pltpu.make_async_copy(
                self.source(kind, start),
                self.target(kind, self.place.fs, self.place.tp),
                self.local.at[kind],
            )
            self.when(kind, long, here.wait)
            for mask in range(8):
                def arrived(kind=kind, mask=mask):
                    target = self.target(kind, xor(self.place.fs, mask), 1 - self.place.tp)
                    remote(
                        target, target, self.pass_send.at[kind, mask],
                        self.pass_recv.at[kind, mask], self.place.sibling,
                    ).wait_recv()

                self.when(kind, other, arrived)

    def drain(self):
        _, long = self.shares.of(self.place, self.quarter, self.place.tp)
        start, _ = self.shares.of(self.place, self.quarter, self.place.tp)
        for kind in range(self.kinds):
            for mask in range(8):
                if mask:
                    sent, copy = self.out(kind, mask)
                    self.when(kind, sent, copy.wait_send)
                source = self.source(kind, start) if mask == 0 else None
                self.when(kind, long, self.passed(kind, mask, source).wait_send)


class Gather:
    def __init__(self, place, tokens, cut, send, recv):
        self.place, self.tokens, self.cut = place, tokens, cut
        self.send, self.recv = send, recv
        self.half = tokens.shape[0] // 8

    def copy(self, index):
        place, width = self.place, self.tokens.shape[1]
        left, right = pl.ds(0, self.cut), pl.ds(self.cut, width - self.cut)
        mask, columns, peer = (
            (0, pl.ds(0, width), place.z_peer),
            (0, pl.ds(0, width), place.y_peer),
            (1, pl.ds(0, width), place.y_peer),
            (0, pl.ds(0, width), place.x_peer),
            (1, pl.ds(0, width), place.x_peer),
            (2, left, place.x_peer),
            (3, left, place.x_peer),
            (4, right, place.y_peer),
            (5, right, place.y_peer),
        )[index]
        block = self.tokens.at[rows_at(place.member(mask), self.half), columns]
        return remote(block, block, self.send.at[index], self.recv.at[index], peer)

    def arrival(self, index):
        place, width = self.place, self.tokens.shape[1]
        left, right = pl.ds(0, self.cut), pl.ds(self.cut, width - self.cut)
        mask, columns = (
            (1, pl.ds(0, width)),
            (2, pl.ds(0, width)),
            (3, pl.ds(0, width)),
            (4, pl.ds(0, width)),
            (5, pl.ds(0, width)),
            (6, left),
            (7, left),
            (6, right),
            (7, right),
        )[index]
        block = self.tokens.at[rows_at(place.member(mask), self.half), columns]
        remote(block, block, self.send.at[index], self.recv.at[index], place.x_peer).wait_recv()


class Scatter:
    def __init__(self, place, part, cut, relay, from_x, from_y, send_z, from_z, send, recv):
        self.place, self.part, self.cut = place, part, cut
        self.relay, self.from_x, self.from_y = relay, from_x, from_y
        self.send_z, self.from_z = send_z, from_z
        self.send, self.recv = send, recv
        self.half = part.shape[0] // 8
        width = part.shape[1]
        self.left, self.right = pl.ds(0, cut), pl.ds(cut, width - cut)

    def block(self, turn, mask):
        return rows_at(self.place.member(2 * mask + 1 - turn), self.half)

    def copy(self, turn, index):
        place = self.place
        mask, columns, target, peer = (
            (3, self.left, self.relay, place.x_peer),
            (3, self.right, self.relay, place.y_peer),
            (2, self.left, self.from_x, place.x_peer),
            (1, self.right, self.from_y, place.y_peer),
            (1, self.left, self.from_y, place.y_peer),
            (2, self.right, self.from_x, place.x_peer),
        )[index]
        return remote(
            self.part.at[self.block(turn, mask), columns],
            target.at[pl.ds(turn * self.half, self.half), columns],
            self.send.at[turn, index],
            self.recv.at[turn, index],
            peer,
        )

    def add(self, turn, index):
        columns, mask = ((self.left, 1), (self.right, 2))[index]
        self.copy(turn, index).wait_recv()
        rows = self.block(turn, mask)
        got = self.relay[pl.ds(turn * self.half, self.half), columns]
        mine = self.part[rows, columns]
        total = mine.astype(jnp.float32) + got.astype(jnp.float32)
        self.part[rows, columns] = total.astype(self.part.dtype)
        self.copy(turn, 4 + index).start()

    def total(self, turn):
        for index in range(2, 6):
            self.copy(turn, index).wait_recv()
        rows = pl.ds(turn * self.half, self.half)
        result = self.part[self.block(turn, 0), :].astype(jnp.float32)
        result = result + self.from_x[rows, :].astype(jnp.float32)
        return result + self.from_y[rows, :].astype(jnp.float32)

    def z_copy(self):
        return remote(
            self.send_z, self.from_z, self.send.at[2, 0], self.recv.at[2, 0], self.place.z_peer
        )

    def drain(self):
        for turn in range(2):
            for index in range(6):
                self.copy(turn, index).wait_send()
        self.z_copy().wait_send()


def product(left, right):
    return jnp.dot(left, right, preferred_element_type=jnp.float32)


def ffn_stage(place, gather, weights, scatter, early):
    kinds = weights.kinds
    near, far = (1, 2, 3), (4, 5, 6, 7)
    rest = [(kind, mask) for kind in range(kinds) for mask in far + near]
    rest = [piece for piece in rest if piece not in early]
    for index in (0, 1, 3):
        gather.copy(index).start()
    third = len(rest) // 3
    weights.start(rest[:third])
    gather.arrival(0)
    gather.copy(2).start()
    gather.copy(4).start()
    weights.start(rest[third:])
    for index, relays in ((1, 5), (3, 7), (2, 6), (4, 8)):
        gather.arrival(index)
        gather.copy(relays).start()
    weights.forward(early + rest)
    for index in range(5, 9):
        gather.arrival(index)
    weights.finish()
    gate, up, down = weights.whole
    size = 2 * gather.half

    def quadrant(step, carry):
        @pl.when(step == 3)
        def relay():
            scatter.add(0, 0)
            scatter.add(0, 1)

        mask = 3 - step
        rep = lax.rem(place.rep + lax.div(mask, jnp.int32(2)), 2)
        y = lax.rem(place.y + lax.rem(mask, 2), 2)
        rows = rows_at(2 * rep + y, size)
        tokens = gather.tokens[rows, :]
        hidden = (
            jax.nn.silu(product(tokens, gate[...])) * product(tokens, up[...])
        ).astype(jnp.bfloat16)
        scatter.part[rows, :] = product(hidden, down[...]).astype(jnp.bfloat16)

        for which, indices in ((0, (0, 1)), (1, (2,)), (2, (3,))):
            def send(indices=indices):
                for turn in range(2):
                    for index in indices:
                        scatter.copy(turn, index).start()

            pl.when(step == which)(send)
        return carry

    lax.fori_loop(0, 4, quadrant, jnp.int32(0))
    scatter.add(1, 0)
    scatter.add(1, 1)
    scatter.send_z[...] = scatter.total(0).astype(jnp.bfloat16)
    scatter.z_copy().start()
    result = scatter.total(1)
    scatter.z_copy().wait_recv()
    return result + scatter.from_z[...].astype(jnp.float32)


def ffn_scratch(half, width, shares):
    token = lambda rows: VMEM((rows * half, width), jnp.bfloat16)
    sems = pltpu.SemaphoreType.DMA
    kinds = 6 if shares.extra else 3
    return [
        token(8),
        VMEM((width, 2 * shares.slot), jnp.bfloat16),
        VMEM((width, 2 * shares.slot), jnp.bfloat16),
        VMEM((2 * shares.slot, width), jnp.bfloat16),
        token(8), token(2), token(2), token(2), token(1), token(1),
        sems((9,)), sems((9,)),
        sems((kinds, 8)), sems((kinds, 8)), sems((kinds, 8)), sems((kinds, 8)), sems((kinds,)),
        sems((3, 6)), sems((3, 6)),
    ]


def ffn_parts(place, shares, shards, scratch, cut):
    (tokens, gate, up, down, part, relay, from_x, from_y, send_z, from_z,
     ag_send, ag_recv, w_send, w_recv, p_send, p_recv, w_local, rs_send, rs_recv) = scratch
    gather = Gather(place, tokens, cut, ag_send, ag_recv)
    weights = Weights(
        place, shares, shards, (gate, up, down), (w_send, w_recv, p_send, p_recv, w_local)
    )
    scatter = Scatter(
        place, part, cut, relay, from_x, from_y, send_z, from_z, rs_send, rs_recv
    )
    return gather, weights, scatter


FAR_GATE = [(0, mask) for mask in (4, 5, 6, 7)]
FAR_UP = [(1, mask) for mask in (4, 5, 6, 7)]


def kernel_one(shares, cut, stream, gain, gate, up, down, out, mine, send, recv, local, *scratch):
    place = Place()
    gather, weights, scatter = ffn_parts(place, shares, (gate, up, down), scratch, cut)
    half, _ = out.shape
    share = stream.shape[1]
    place.barrier()
    columns = rows_at(place.tp, share)
    there = remote(
        stream.at[rows_at(1 - place.tp, half), :], mine.at[:, columns],
        send.at[0], recv.at[0], place.sibling,
    )
    here = pltpu.make_async_copy(
        stream.at[rows_at(place.tp, half), :], mine.at[:, columns], local.at[0]
    )
    there.start()
    here.start()
    weights.start(FAR_GATE)
    weights.own()
    weights.blank()
    here.wait()
    there.wait_recv()
    normed = rms_scale(mine[...].astype(jnp.float32), gain[...])
    gather.tokens[rows_at(place.member(0), half), :] = normed.astype(jnp.bfloat16)
    total = ffn_stage(place, gather, weights, scatter, FAR_GATE)
    out[...] = (mine[...].astype(jnp.float32) + 0.5 * total).astype(jnp.bfloat16)
    there.wait_send()
    for index in range(9):
        gather.copy(index).wait_send()
    weights.drain()
    scatter.drain()


def kernel_two(
    shares, cut, first, gains, proj_u, proj_v, proj_out, spatial, bias, mix_gain, head_gain,
    gate, up, down, out, pu, pv, po, mixed_rows, gated, terms, other, second, result,
    send, recv, local, *scratch
):
    place = Place()
    gather, weights, scatter = ffn_parts(place, shares, (gate, up, down), scratch, cut)
    half, _ = first.shape
    share = out.shape[1]
    fetch = [
        pltpu.make_async_copy(source, target, local.at[index])
        for index, (source, target) in enumerate(((proj_u, pu), (proj_v, pv), (proj_out, po)))
    ]
    for copy in fetch:
        copy.start()
    place.barrier()
    weights.start(FAR_GATE + FAR_UP)
    weights.own()
    weights.blank()
    own, sibling = rows_at(place.tp, half), rows_at(1 - place.tp, half)
    normed = rms_scale(first[...].astype(jnp.float32), gains[0:1, :])
    mixed_rows[own, :] = normed.astype(jnp.bfloat16)
    trade = remote(
        mixed_rows.at[own, :], mixed_rows.at[own, :], send.at[0], recv.at[0], place.sibling
    )
    trade.start()
    for copy in fetch:
        copy.wait()
    trade_in = remote(
        mixed_rows.at[sibling, :], mixed_rows.at[sibling, :], send.at[0], recv.at[0], place.sibling
    )
    trade_in.wait_recv()
    row = lax.broadcasted_iota(jnp.int32, (BLOCK, BLOCK), 0) // SPAN
    column = lax.broadcasted_iota(jnp.int32, (BLOCK, BLOCK), 1) // SPAN
    causal = row >= column
    u_part = jax.nn.gelu(product(mixed_rows[...], pu[...]))
    v_part = jax.nn.gelu(product(mixed_rows[...], pv[...]))
    for head in range(spatial.shape[0]):
        at = slice(head * HEAD_DIM, (head + 1) * HEAD_DIM)
        matrix = jnp.where(causal, spatial[head], jnp.zeros_like(spatial[head]))
        for start in range(0, 2 * half, BLOCK):
            rows = slice(start, start + BLOCK)
            value = v_part[rows, at]
            centred = value - jnp.mean(value, axis=-1, keepdims=True)
            spread = jnp.mean(jnp.square(centred), axis=-1, keepdims=True)
            vn = (centred * lax.rsqrt(spread + 1e-05) * mix_gain[:, at]).astype(jnp.bfloat16)
            mixed = product(matrix, vn) + bias[:, head : head + 1]
            gated[rows, at] = rms_scale(u_part[rows, at] * mixed, head_gain[:, at]).astype(
                jnp.bfloat16
            )
    for part in range(po.shape[0]):
        at = pl.ds(part * po.shape[2], po.shape[2])
        terms[:, at] = product(gated[...], po[part]).astype(jnp.bfloat16)
    swap = remote(terms.at[sibling, :], other, send.at[1], recv.at[1], place.sibling)
    swap.start()
    swap.wait_recv()
    branch = terms[own, :].astype(jnp.float32) + other[...].astype(jnp.float32)
    second[...] = (first[...].astype(jnp.float32) + branch).astype(jnp.bfloat16)
    normed = rms_scale(second[...].astype(jnp.float32), gains[1:2, :])
    gather.tokens[rows_at(place.member(0), half), :] = normed.astype(jnp.bfloat16)
    total = ffn_stage(place, gather, weights, scatter, FAR_GATE + FAR_UP)
    result[...] = (second[...].astype(jnp.float32) + 0.5 * total).astype(jnp.bfloat16)
    there = remote(
        result.at[:, rows_at(1 - place.tp, share)], out.at[own, :],
        send.at[2], recv.at[2], place.sibling,
    )
    there.start()
    here = pltpu.make_async_copy(
        result.at[:, rows_at(place.tp, share)], out.at[own, :], local.at[0]
    )
    here.start()
    trade.wait_send()
    swap.wait_send()
    for index in range(9):
        gather.copy(index).wait_send()
    weights.drain()
    scatter.drain()
    there.wait_send()
    here.wait()
    remote(
        result.at[:, rows_at(1 - place.tp, share)], out.at[sibling, :],
        send.at[2], recv.at[2], place.sibling,
    ).wait_recv()


ANY = pl.BlockSpec(memory_space=pl.ANY)
WHOLE = pl.BlockSpec(memory_space=pltpu.VMEM)


def params(collective_id):
    return pltpu.CompilerParams(
        collective_id=collective_id, has_side_effects=True, vmem_limit_bytes=62 * 2**20
    )


def estimate(units, width, tokens):
    return pl.CostEstimate(
        flops=6 * tokens * units * width, bytes_accessed=64 * units * width, transcendentals=0
    )


def first_block(stream, gain, gate_weight, up_weight, down_weight):
    half, width = stream.shape[0] // 2, stream.shape[1] * lax.axis_size("tp")
    shares = Shares(gate_weight.shape[1])
    sems = pltpu.SemaphoreType.DMA
    return pl.pallas_call(
        functools.partial(kernel_one, shares, width // 2),
        out_shape=jax.ShapeDtypeStruct((half, width), jnp.bfloat16),
        in_specs=[ANY, WHOLE, ANY, ANY, ANY],
        out_specs=WHOLE,
        scratch_shapes=[
            VMEM((half, width), jnp.bfloat16), sems((1,)), sems((1,)), sems((1,)),
        ] + ffn_scratch(half, width, shares),
        compiler_params=params(1),
        cost_estimate=estimate(gate_weight.shape[1], width, stream.shape[0]),
    )(stream, gain[None], gate_weight, up_weight, down_weight)


def second_block(first, gains, projections, mixing, weights):
    half, width = first.shape
    shares = Shares(weights[0].shape[1])
    sems = pltpu.SemaphoreType.DMA
    channels = projections[0].shape[1]
    bf16 = jnp.bfloat16
    return pl.pallas_call(
        functools.partial(kernel_two, shares, width // 2),
        out_shape=jax.ShapeDtypeStruct((2 * half, width // 2), bf16),
        in_specs=[WHOLE, WHOLE, ANY, ANY, ANY, WHOLE, WHOLE, WHOLE, WHOLE, ANY, ANY, ANY],
        out_specs=ANY,
        scratch_shapes=[
            VMEM((width, channels), bf16),
            VMEM((width, channels), bf16),
            VMEM(projections[2].shape, bf16),
            VMEM((2 * half, width), bf16),
            VMEM((2 * half, channels), bf16),
            VMEM((2 * half, width), bf16),
            VMEM((half, width), bf16),
            VMEM((half, width), bf16),
            VMEM((half, width), bf16),
            sems((3,)), sems((3,)), sems((3,)),
        ] + ffn_scratch(half, width, shares),
        compiler_params=params(2),
        cost_estimate=estimate(weights[0].shape[1], width, 2 * half),
    )(first, gains, *projections, *mixing, *weights)


def cubes(stream, gate_weight):
    sizes = tuple(lax.axis_size(name) for name in ("rep", "fs", "tp"))
    rows, units = gate_weight.shape
    width = stream.shape[1] * 2
    return (
        sizes == (2, 8, 2)
        and stream.shape[0] % (2 * BLOCK) == 0
        and stream.shape[1] % (2 * LANE) == 0
        and units % (2 * LANE) == 0
        and units >= 16 * LANE
        and rows % 32 == 0
        and width * (6 * units // 8 + 22 * stream.shape[0] // 2 + 3 * 512) * 2 < 48 * 2**20
    )


def feed_forward(stream, gain, gate_weight, up_weight, down_weight):
    normed = normalized(stream, gain)
    gate, up_part = ffn_inputs(normed, gate_weight, up_weight)
    hidden = (jax.nn.silu(gate) * up_part).astype(jnp.bfloat16)
    terms = jnp.dot(
        hidden,
        lax.all_gather(down_weight, "fs", axis=1, tiled=True),
        preferred_element_type=jnp.float32,
    )
    return lax.psum_scatter(
        terms.astype(jnp.bfloat16), "tp", scatter_dimension=1, tiled=True
    ).astype(jnp.float32)


def body(
    resid,
    norm_gains,
    gate_one,
    up_one,
    down_one,
    proj_u,
    proj_v,
    spatial,
    spatial_bias,
    mix_gain,
    head_gain,
    proj_out,
    gate_two,
    up_two,
    down_two,
):
    if cubes(resid, gate_one):
        whole_u = lax.all_gather(proj_u, "fs", axis=0, tiled=True)
        whole_v = lax.all_gather(proj_v, "fs", axis=0, tiled=True)
        whole_out = lax.all_gather(proj_out, "fs", axis=0)
        first = first_block(resid, norm_gains[0], gate_one, up_one, down_one)
        return second_block(
            first, norm_gains[1:], (whole_u, whole_v, whole_out),
            (spatial, spatial_bias.T, mix_gain[None], head_gain[None]),
            (gate_two, up_two, down_two),
        )
    total = feed_forward(resid, norm_gains[0], gate_one, up_one, down_one)
    first = (resid.astype(jnp.float32) + 0.5 * total).astype(jnp.bfloat16)
    mnormed = normalized(first, norm_gains[1])
    u_part, v_part = mixer_inputs(mnormed, proj_u, proj_v)
    proj_out = lax.all_gather(proj_out, "fs", axis=1, tiled=True)
    rows = u_part.shape[0]
    seqs = rows // BLOCK
    local_heads = spatial.shape[0]
    gated_u = jax.nn.gelu(u_part).reshape(seqs, BLOCK, local_heads, HEAD_DIM)
    gated_v = jax.nn.gelu(v_part).reshape(seqs, BLOCK, local_heads, HEAD_DIM)
    centre = jnp.mean(gated_v, axis=-1, keepdims=True)
    spread = jnp.mean(jnp.square(gated_v - centre), axis=-1, keepdims=True)
    vn = (
        (gated_v - centre) * lax.rsqrt(spread + 1e-05) * mix_gain.reshape(local_heads, HEAD_DIM)
    ).astype(jnp.bfloat16)
    segment = jnp.arange(BLOCK) // SPAN
    causal = segment[:, None] >= segment[None, :]
    masked = jnp.where(causal[None], spatial, jnp.zeros_like(spatial))
    mixed = (
        jnp.einsum("hts,bshd->bthd", masked, vn, preferred_element_type=jnp.float32)
        + spatial_bias.T[None, :, :, None]
    )
    product = gated_u * mixed
    gated = (
        rms_scale(product, head_gain.reshape(local_heads, HEAD_DIM))
        .astype(jnp.bfloat16)
        .reshape(rows, local_heads * HEAD_DIM)
    )
    terms = jnp.dot(
        gated,
        proj_out,
        preferred_element_type=jnp.float32,
    )
    branch = lax.psum_scatter(
        terms.astype(jnp.bfloat16), "tp", scatter_dimension=1, tiled=True
    ).astype(jnp.float32)
    second = (first.astype(jnp.float32) + branch).astype(jnp.bfloat16)
    total = feed_forward(second, norm_gains[2], gate_two, up_two, down_two)
    return (second.astype(jnp.float32) + 0.5 * total).astype(jnp.bfloat16)


def solution(mesh):
    return jax.shard_map(
        body,
        mesh=mesh,
        in_specs=(
            P(("rep", "fs"), "tp"),
            P(),
            P("fs", "tp"),
            P("fs", "tp"),
            P("tp", "fs"),
            P("fs", "tp"),
            P("fs", "tp"),
            P("tp", None, None),
            P("tp", None),
            P("tp"),
            P("tp"),
            P("tp", "fs"),
            P("fs", "tp"),
            P("fs", "tp"),
            P("tp", "fs"),
        ),
        out_specs=P(("rep", "fs"), "tp"),
        check_vma=False,
    )
```

```python
import functools

import jax
import jax.numpy as jnp
from jax import lax
from jax.experimental import pallas as pl
from jax.experimental.pallas import tpu as pltpu
from jax.sharding import PartitionSpec as P

HEAD_DIM = 128
BLOCK = 128
SPAN = 64


def rms_scale(values, gain):
    return values * lax.rsqrt(jnp.mean(values * values, axis=-1, keepdims=True) + 1e-06) * gain


def normalized(stream, gain):
    whole = lax.all_gather(stream, "tp", axis=1, tiled=True).astype(jnp.float32)
    return rms_scale(whole, gain).astype(jnp.bfloat16)


def accumulate(left, piece):
    return jnp.dot(left, piece, preferred_element_type=jnp.float32)


def folders(normed):

    def single(total, piece, start):
        return accumulate(normed, piece)

    def double(totals, pieces, start):
        return (accumulate(normed, pieces[0]), accumulate(normed, pieces[1]))

    return (single, double)


def ffn_inputs(normed, first_weight, second_weight):
    empty = jnp.zeros((normed.shape[0], first_weight.shape[1]), jnp.float32)
    single, _ = folders(normed)
    result = (
        single(empty, lax.all_gather(first_weight, "fs", axis=0, tiled=True), jnp.int32(0)),
        single(empty, lax.all_gather(second_weight, "fs", axis=0, tiled=True), jnp.int32(0)),
    )
    return result


def mixer_inputs(normed, first_weight, second_weight):
    empty = jnp.zeros((normed.shape[0], first_weight.shape[1]), jnp.float32)
    single, _ = folders(normed)
    result = (
        single(empty, lax.all_gather(first_weight, "fs", axis=0, tiled=True), jnp.int32(0)),
        single(empty, lax.all_gather(second_weight, "fs", axis=0, tiled=True), jnp.int32(0)),
    )
    return result


LANE = 128
MESH = pl.DeviceIdType.MESH
VMEM = pltpu.VMEM


def flip(value, bit):
    return value + bit - 2 * bit * lax.rem(lax.div(value, jnp.int32(bit)), 2)


def xor(value, mask):
    for bit in (1, 2, 4):
        if mask & bit:
            value = flip(value, bit)
    return value


class Place:
    def __init__(self):
        self.rep, self.fs, self.tp = (lax.axis_index(name) for name in ("rep", "fs", "tp"))
        self.y = lax.rem(self.fs, 2)
        self.z = lax.rem(lax.div(self.fs, jnp.int32(2)), 2)
        self.x_peer = {"rep": 1 - self.rep}
        self.y_peer = {"fs": flip(self.fs, 1)}
        self.z_peer = {"fs": flip(self.fs, 2)}
        self.sibling = {"tp": 1 - self.tp}

    def member(self, mask):
        return xor(4 * self.rep + 2 * self.y + self.z, mask)

    def barrier(self):
        semaphore = pltpu.get_barrier_semaphore()
        peers = [{"fs": xor(self.fs, mask)} for mask in range(1, 8)]
        peers += [self.x_peer, self.sibling]
        for peer in peers:
            pl.semaphore_signal(semaphore, inc=1, device_id=peer, device_id_type=MESH)
        pl.semaphore_wait(semaphore, len(peers))


def remote(src, dst, send, recv, peer):
    return pltpu.make_async_remote_copy(
        src_ref=src, dst_ref=dst, send_sem=send, recv_sem=recv,
        device_id=peer, device_id_type=MESH,
    )


def rows_at(index, size):
    return pl.ds(pl.multiple_of(index * size, size), size)


class Shares:
    def __init__(self, units):
        self.tiles = units // LANE // 2
        self.most = -(-self.tiles // 4)
        self.missing = 4 * self.most - self.tiles
        self.base = (self.most - (1 if self.missing else 0)) * LANE
        self.extra = LANE if self.missing else 0
        self.slot = self.most * LANE

    def of(self, place, quarter, core):
        late = 4 - self.missing
        before = jnp.where(
            core == 0, jnp.maximum(quarter - late, 0), jnp.minimum(quarter, self.missing)
        )
        long = jnp.where(core == 0, quarter < late, quarter >= self.missing)
        start = place.rep * self.tiles + quarter * self.most - before
        return start * LANE, long


class Weights:
    def __init__(self, place, shares, shards, whole, sems):
        self.place, self.shares, self.shards, self.whole = place, shares, shards, whole
        self.send_sem, self.recv_sem, self.pass_send, self.pass_recv, self.local = sems
        self.kinds = 6 if shares.extra else 3
        self.quarter = lax.rem(place.fs, 4)

    def source(self, kind, start):
        shares, which = self.shares, kind % 3
        first = start + (shares.base if kind >= 3 else 0)
        size = shares.extra if kind >= 3 else shares.base
        ref = self.shards[which]
        first = jnp.minimum(first, ref.shape[0 if which == 2 else 1] - size)
        cut = pl.ds(pl.multiple_of(first, LANE), size)
        return ref.at[cut, :] if which == 2 else ref.at[:, cut]

    def target(self, kind, owner, core):
        shares, which = self.shares, kind % 3
        first = core * shares.slot + (shares.base if kind >= 3 else 0)
        size = shares.extra if kind >= 3 else shares.base
        cut = pl.ds(pl.multiple_of(first, LANE), size)
        ref = self.whole[which]
        if which == 2:
            return ref.at[cut, rows_at(owner, self.shards[2].shape[1])]
        return ref.at[rows_at(owner, self.shards[which].shape[0]), cut]

    def when(self, kind, long, action):
        if kind >= 3:
            pl.when(long)(action)
        else:
            action()

    def out(self, kind, mask):
        peer = xor(self.place.fs, mask)
        start, long = self.shares.of(self.place, lax.rem(peer, 4), self.place.tp)
        return long, remote(
            self.source(kind, start),
            self.target(kind, self.place.fs, self.place.tp),
            self.send_sem.at[kind, mask],
            self.recv_sem.at[kind, mask],
            {"fs": peer},
        )

    def start(self, pieces):
        for kind, mask in pieces:
            long, copy = self.out(kind, mask)
            self.when(kind, long, copy.start)

    def own(self):
        start, long = self.shares.of(self.place, self.quarter, self.place.tp)
        for kind in range(self.kinds):
            source = self.source(kind, start)
            target = self.target(kind, self.place.fs, self.place.tp)
            here = pltpu.make_async_copy(source, target, self.local.at[kind])
            there = self.passed(kind, 0, source)

            def begin(here=here, there=there):
                here.start()
                there.start()

            self.when(kind, long, begin)

    def passed(self, kind, mask, source=None):
        target = self.target(kind, xor(self.place.fs, mask), self.place.tp)
        return remote(
            target if source is None else source,
            target,
            self.pass_send.at[kind, mask],
            self.pass_recv.at[kind, mask],
            self.place.sibling,
        )

    def blank(self):
        shares = self.shares
        if not shares.extra:
            return
        for core in range(2):
            _, long = shares.of(self.place, self.quarter, core)
            cut = pl.ds(core * shares.slot + shares.base, shares.extra)

            def clear(cut=cut):
                for ref in self.whole[:2]:
                    ref[:, cut] = jnp.zeros((ref.shape[0], shares.extra), ref.dtype)
                down = self.whole[2]
                down[cut, :] = jnp.zeros((shares.extra, down.shape[1]), down.dtype)

            pl.when(jnp.logical_not(long))(clear)

    def forward(self, pieces):
        _, long = self.shares.of(self.place, self.quarter, self.place.tp)
        for kind, mask in pieces:
            def step(kind=kind, mask=mask):
                self.out(kind, mask)[1].wait_recv()
                self.passed(kind, mask).start()

            self.when(kind, long, step)

    def finish(self):
        _, long = self.shares.of(self.place, self.quarter, self.place.tp)
        _, other = self.shares.of(self.place, self.quarter, 1 - self.place.tp)
        start, _ = self.shares.of(self.place, self.quarter, self.place.tp)
        for kind in range(self.kinds):
            here = pltpu.make_async_copy(
                self.source(kind, start),
                self.target(kind, self.place.fs, self.place.tp),
                self.local.at[kind],
            )
            self.when(kind, long, here.wait)
            for mask in range(8):
                def arrived(kind=kind, mask=mask):
                    target = self.target(kind, xor(self.place.fs, mask), 1 - self.place.tp)
                    remote(
                        target, target, self.pass_send.at[kind, mask],
                        self.pass_recv.at[kind, mask], self.place.sibling,
                    ).wait_recv()

                self.when(kind, other, arrived)

    def drain(self):
        _, long = self.shares.of(self.place, self.quarter, self.place.tp)
        start, _ = self.shares.of(self.place, self.quarter, self.place.tp)
        for kind in range(self.kinds):
            for mask in range(8):
                if mask:
                    sent, copy = self.out(kind, mask)
                    self.when(kind, sent, copy.wait_send)
                source = self.source(kind, start) if mask == 0 else None
                self.when(kind, long, self.passed(kind, mask, source).wait_send)


class Gather:
    def __init__(self, place, tokens, cut, send, recv):
        self.place, self.tokens, self.cut = place, tokens, cut
        self.send, self.recv = send, recv
        self.half = tokens.shape[0] // 8

    def copy(self, index):
        place, width = self.place, self.tokens.shape[1]
        left, right = pl.ds(0, self.cut), pl.ds(self.cut, width - self.cut)
        mask, columns, peer = (
            (0, pl.ds(0, width), place.z_peer),
            (0, pl.ds(0, width), place.y_peer),
            (1, pl.ds(0, width), place.y_peer),
            (0, pl.ds(0, width), place.x_peer),
            (1, pl.ds(0, width), place.x_peer),
            (2, left, place.x_peer),
            (3, left, place.x_peer),
            (4, right, place.y_peer),
            (5, right, place.y_peer),
        )[index]
        block = self.tokens.at[rows_at(place.member(mask), self.half), columns]
        return remote(block, block, self.send.at[index], self.recv.at[index], peer)

    def arrival(self, index):
        place, width = self.place, self.tokens.shape[1]
        left, right = pl.ds(0, self.cut), pl.ds(self.cut, width - self.cut)
        mask, columns = (
            (1, pl.ds(0, width)),
            (2, pl.ds(0, width)),
            (3, pl.ds(0, width)),
            (4, pl.ds(0, width)),
            (5, pl.ds(0, width)),
            (6, left),
            (7, left),
            (6, right),
            (7, right),
        )[index]
        block = self.tokens.at[rows_at(place.member(mask), self.half), columns]
        remote(block, block, self.send.at[index], self.recv.at[index], place.x_peer).wait_recv()

    def drain(self):
        for index in range(9):
            self.copy(index).wait_send()


class Scatter:
    def __init__(self, place, part, cut, relay, from_x, from_y, send_z, from_z, send, recv):
        self.place, self.part, self.cut = place, part, cut
        self.relay, self.from_x, self.from_y = relay, from_x, from_y
        self.send_z, self.from_z = send_z, from_z
        self.send, self.recv = send, recv
        self.half = part.shape[0] // 8
        width = part.shape[1]
        self.left, self.right = pl.ds(0, cut), pl.ds(cut, width - cut)

    def block(self, turn, mask):
        return rows_at(self.place.member(2 * mask + 1 - turn), self.half)

    def copy(self, turn, index):
        place = self.place
        mask, columns, target, peer = (
            (3, self.left, self.relay, place.x_peer),
            (3, self.right, self.relay, place.y_peer),
            (2, self.left, self.from_x, place.x_peer),
            (1, self.right, self.from_y, place.y_peer),
            (1, self.left, self.from_y, place.y_peer),
            (2, self.right, self.from_x, place.x_peer),
        )[index]
        return remote(
            self.part.at[self.block(turn, mask), columns],
            target.at[pl.ds(turn * self.half, self.half), columns],
            self.send.at[turn, index],
            self.recv.at[turn, index],
            peer,
        )

    def add(self, turn, index):
        columns, mask = ((self.left, 1), (self.right, 2))[index]
        self.copy(turn, index).wait_recv()
        rows = self.block(turn, mask)
        got = self.relay[pl.ds(turn * self.half, self.half), columns]
        mine = self.part[rows, columns]
        total = mine.astype(jnp.float32) + got.astype(jnp.float32)
        self.part[rows, columns] = total.astype(self.part.dtype)
        self.copy(turn, 4 + index).start()

    def total(self, turn):
        for index in range(2, 6):
            self.copy(turn, index).wait_recv()
        rows = pl.ds(turn * self.half, self.half)
        result = self.part[self.block(turn, 0), :].astype(jnp.float32)
        result = result + self.from_x[rows, :].astype(jnp.float32)
        return result + self.from_y[rows, :].astype(jnp.float32)

    def z_copy(self):
        return remote(
            self.send_z, self.from_z, self.send.at[2, 0], self.recv.at[2, 0], self.place.z_peer
        )

    def drain(self):
        for turn in range(2):
            for index in range(6):
                self.copy(turn, index).wait_send()
        self.z_copy().wait_send()


def product(left, right):
    return jnp.dot(left, right, preferred_element_type=jnp.float32)


def gather_start(gather):
    for index in (0, 1, 3):
        gather.copy(index).start()


def gather_near(gather):
    gather.arrival(0)
    gather.copy(2).start()
    gather.copy(4).start()


def gather_relay(gather):
    for index, relays in ((1, 5), (3, 7), (2, 6), (4, 8)):
        gather.arrival(index)
        gather.copy(relays).start()


def gather_finish(gather):
    for index in range(5, 9):
        gather.arrival(index)


def block_sums(place, gather, weights, scatter, soon, later):
    gate, up, down = weights.whole
    size = 2 * gather.half

    def quadrant(step, carry):
        @pl.when(step == 3)
        def relay():
            scatter.add(0, 0)
            scatter.add(0, 1)
            for index in (0, 2, 3):
                scatter.copy(1, index).start()

        mask = 3 - step
        rep = lax.rem(place.rep + lax.div(mask, jnp.int32(2)), 2)
        y = lax.rem(place.y + lax.rem(mask, 2), 2)
        rows = rows_at(2 * rep + y, size)
        tokens = gather.tokens[rows, :]
        hidden = (
            jax.nn.silu(product(tokens, gate[...])) * product(tokens, up[...])
        ).astype(jnp.bfloat16)
        scatter.part[rows, :] = product(hidden, down[...]).astype(jnp.bfloat16)

        for which, copies in ((0, ((0, 0), (0, 1), (1, 1))), (1, ((0, 2),)), (2, ((0, 3),))):
            def send(copies=copies):
                for turn, index in copies:
                    scatter.copy(turn, index).start()

            pl.when(step == which)(send)
        return carry

    lax.fori_loop(0, 4, quadrant, jnp.int32(0))
    gather.drain()
    soon()
    scatter.add(1, 0)
    scatter.add(1, 1)
    later()
    scatter.send_z[...] = scatter.total(0).astype(jnp.bfloat16)
    scatter.z_copy().start()
    result = scatter.total(1)
    scatter.z_copy().wait_recv()
    return result + scatter.from_z[...].astype(jnp.float32)


class Mixing:
    SLOTS = tuple(
        [("far", 0)]
        + [("z", mask) for mask in (0, 4)]
        + [("y", mask) for mask in (0, 4, 2, 6)]
        + [("x", mask) for mask in (4, 2, 6, 1, 5, 3, 7)]
    )

    def __init__(self, place, shards, whole, send, recv, local):
        self.place, self.shards, self.whole = place, shards, whole
        self.send, self.recv, self.local = send, recv, local

    def part(self, kind, half):
        size = self.shards[kind].shape[0] // 2
        return self.shards[kind].at[rows_at(half, size), :]

    def target(self, kind, owner, half):
        size = self.shards[kind].shape[0] // 2
        if kind == 2:
            return self.whole[2].at[owner, rows_at(half, size), :]
        return self.whole[kind].at[rows_at(2 * owner + half, size), :]

    def copy(self, kind, slot):
        place = self.place
        way, mask = self.SLOTS[slot]
        peer = {
            "far": {"fs": xor(place.fs, 4)},
            "y": place.y_peer,
            "z": place.z_peer,
            "x": place.x_peer,
        }[way]
        target = self.target(kind, xor(place.fs, mask), place.rep)
        source = target if mask else self.part(kind, place.rep)
        return remote(source, target, self.send.at[kind, slot], self.recv.at[kind, slot], peer)

    def start(self, slots):
        for slot in slots:
            for kind in range(3):
                self.copy(kind, slot).start()

    def arrive(self, slots):
        place = self.place
        for slot in slots:
            way, mask = self.SLOTS[slot]
            mask ^= {"far": 4, "y": 1, "z": 2, "x": 0}[way]
            half = 1 - place.rep if way == "x" else place.rep
            for kind in range(3):
                target = self.target(kind, xor(place.fs, mask), half)
                remote(
                    target, target, self.send.at[kind, slot], self.recv.at[kind, slot],
                    place.x_peer,
                ).wait_recv()

    def own(self):
        copies = []
        for kind in range(3):
            size = self.shards[kind].shape[0]
            target = (
                self.whole[2].at[self.place.fs]
                if kind == 2
                else self.whole[kind].at[rows_at(self.place.fs, size), :]
            )
            copies.append(
                pltpu.make_async_copy(self.shards[kind], target, self.local.at[kind])
            )
        return copies

    def drain(self):
        for slot in range(len(self.SLOTS)):
            for kind in range(3):
                self.copy(kind, slot).wait_send()


def mix(place, first, normed_rows, projections, mixing, gated, terms, other, send, recv):
    spatial, bias, mix_gain, head_gain = mixing
    pu, pv, po = projections
    half = first.shape[0]
    own, sibling = rows_at(place.tp, half), rows_at(1 - place.tp, half)
    remote(
        normed_rows.at[sibling, :], normed_rows.at[sibling, :], send.at[1], recv.at[1],
        place.sibling,
    ).wait_recv()
    row = lax.broadcasted_iota(jnp.int32, (BLOCK, BLOCK), 0)
    column = lax.broadcasted_iota(jnp.int32, (BLOCK, BLOCK), 1)
    causal = lax.div(row, SPAN) >= lax.div(column, SPAN)
    u_part = jax.nn.gelu(product(normed_rows[...], pu[...]))
    v_part = jax.nn.gelu(product(normed_rows[...], pv[...]))
    for head in range(spatial.shape[0]):
        at = slice(head * HEAD_DIM, (head + 1) * HEAD_DIM)
        matrix = jnp.where(causal, spatial[head], jnp.zeros_like(spatial[head]))
        shift = jnp.sum(
            jnp.where(row == column, bias[head : head + 1, :], 0.0), axis=1, keepdims=True
        )
        for start in range(0, 2 * half, BLOCK):
            rows = slice(start, start + BLOCK)
            value = v_part[rows, at]
            centred = value - jnp.mean(value, axis=-1, keepdims=True)
            spread = jnp.mean(jnp.square(centred), axis=-1, keepdims=True)
            vn = (centred * lax.rsqrt(spread + 1e-05) * mix_gain[:, at]).astype(jnp.bfloat16)
            mixed = product(matrix, vn) + shift
            gated[rows, at] = rms_scale(u_part[rows, at] * mixed, head_gain[:, at]).astype(
                jnp.bfloat16
            )
    for part in range(po.shape[0]):
        at = pl.ds(part * po.shape[2], po.shape[2])
        terms[:, at] = product(gated[...], po[part]).astype(jnp.bfloat16)
    swap = remote(terms.at[sibling, :], other, send.at[2], recv.at[2], place.sibling)
    swap.start()
    swap.wait_recv()
    branch = terms[own, :].astype(jnp.float32) + other[...].astype(jnp.float32)
    return first[...].astype(jnp.float32) + branch


def near_pieces(kinds):
    return [(kind, mask) for kind in kinds for mask in (1, 2, 3)]


def far_pieces(kinds):
    return [(kind, mask) for kind in kinds for mask in (4, 5, 6, 7)]


def layer_kernel(shares, cuts, *refs):
    (stream, gains, gate_one, up_one, down_one, proj_u, proj_v, spatial, bias, mix_gain,
     head_gain, proj_out, gate_two, up_two, down_two, out) = refs[:16]
    (mine, first, second, normed_rows, gated, terms, other, result, pu, pv, po,
     tokens, part, relay, from_x, from_y, send_z, from_z) = refs[16:34]
    send, recv, local, mix_send, mix_recv, mix_local = refs[34:40]
    ag_send, ag_recv, rs_send, rs_recv = refs[40:44]
    place = Place()
    weights, gathers, scatters = [], [], []
    for which, shards in enumerate(((gate_one, up_one, down_one), (gate_two, up_two, down_two))):
        whole, sems = refs[44 + 8 * which : 47 + 8 * which], refs[47 + 8 * which : 52 + 8 * which]
        weights.append(Weights(place, shares, shards, whole, sems))
        gathers.append(Gather(place, tokens, cuts[2 * which], ag_send.at[which], ag_recv.at[which]))
        scatters.append(
            Scatter(place, part, cuts[2 * which + 1], relay, from_x, from_y, send_z, from_z,
                    rs_send.at[which], rs_recv.at[which])
        )
    mixing = Mixing(place, (proj_u, proj_v, proj_out), (pu, pv, po), mix_send, mix_recv, mix_local)
    half, _ = mine.shape
    share = stream.shape[1]
    place.barrier()

    own, sibling = rows_at(place.tp, half), rows_at(1 - place.tp, half)
    columns = rows_at(place.tp, share)
    there = remote(
        stream.at[sibling, :], mine.at[:, columns], send.at[0], recv.at[0], place.sibling
    )
    here = pltpu.make_async_copy(stream.at[own, :], mine.at[:, columns], local.at[0])
    there.start()
    here.start()
    mixing.start((0, 1, 3))
    one, two = weights
    for copy in mixing.own():
        copy.start()
    here.wait()
    there.wait_recv()
    block = rows_at(place.member(0), half)
    normed = rms_scale(mine[...].astype(jnp.float32), gains[0:1, :])
    tokens[block, :] = normed.astype(jnp.bfloat16)
    gather_start(gathers[0])
    extras = (3, 4, 5) if shares.extra else ()
    one.start(far_pieces((0,)))
    one.own()
    one.blank()
    two.blank()
    mixing.arrive((0,))
    mixing.start((2, 4, 7))
    one.start(far_pieces((1,)))
    mixing.arrive((1, 3))
    mixing.start((5, 8, 10))
    gather_near(gathers[0])
    mixing.arrive((2, 4))
    mixing.start((6, 9, 11))
    one.start(far_pieces((2,) + extras))
    one.start(near_pieces((0, 1, 2) + extras))
    gather_relay(gathers[0])
    mixing.arrive((5, 6))
    mixing.start((12, 13))
    one.forward(far_pieces((0, 1, 2) + extras) + near_pieces((0, 1, 2) + extras))
    gather_finish(gathers[0])
    two.start(far_pieces((0,)))
    one.finish()
    total = block_sums(
        place, gathers[0], one, scatters[0],
        lambda: two.start(far_pieces((1,)) + [(kind, 2) for kind in (0, 1, 2)]),
        lambda: two.start(
            far_pieces((2,)) + [(kind, mask) for kind in (0, 1) for mask in (1, 3)]
        ),
    )
    first[...] = (mine[...].astype(jnp.float32) + 0.5 * total).astype(jnp.bfloat16)

    normed = rms_scale(first[...].astype(jnp.float32), gains[1:2, :])
    normed_rows[own, :] = normed.astype(jnp.bfloat16)
    trade = remote(
        normed_rows.at[own, :], normed_rows.at[own, :], send.at[1], recv.at[1], place.sibling
    )
    trade.start()
    two.own()
    for copy in mixing.own():
        copy.wait()
    mixing.arrive(range(7, 14))
    second[...] = mix(
        place, first, normed_rows, (pu, pv, po), (spatial, bias, mix_gain, head_gain),
        gated, terms, other, send, recv,
    ).astype(jnp.bfloat16)
    scatters[0].drain()
    normed = rms_scale(second[...].astype(jnp.float32), gains[2:3, :])
    tokens[block, :] = normed.astype(jnp.bfloat16)
    gather_start(gathers[1])
    gather_near(gathers[1])
    two.start(far_pieces(extras) + [(2, 1), (2, 3)] + near_pieces(extras))
    gather_relay(gathers[1])
    two.forward(far_pieces((0, 1, 2) + extras) + near_pieces((0, 1, 2) + extras))
    gather_finish(gathers[1])
    two.finish()
    total = block_sums(place, gathers[1], two, scatters[1], lambda: None, lambda: None)
    result[...] = (second[...].astype(jnp.float32) + 0.5 * total).astype(jnp.bfloat16)

    last = remote(
        result.at[:, rows_at(1 - place.tp, share)], out.at[own, :],
        send.at[3], recv.at[3], place.sibling,
    )
    last.start()
    keep = pltpu.make_async_copy(
        result.at[:, rows_at(place.tp, share)], out.at[own, :], local.at[0]
    )
    keep.start()
    there.wait_send()
    trade.wait_send()
    remote(terms.at[sibling, :], other, send.at[2], recv.at[2], place.sibling).wait_send()
    mixing.drain()
    one.drain()
    two.drain()
    scatters[1].drain()
    last.wait_send()
    keep.wait()
    remote(
        result.at[:, rows_at(1 - place.tp, share)], out.at[sibling, :],
        send.at[3], recv.at[3], place.sibling,
    ).wait_recv()


def whole_layer(*args):
    stream, gate, proj_u, proj_out = args[0], args[2], args[5], args[11]
    half, width = stream.shape[0] // 2, 2 * stream.shape[1]
    shares = Shares(gate.shape[1])
    channels = proj_u.shape[1]
    kinds = 6 if shares.extra else 3
    parts = lax.axis_size("fs")
    even, wide = width // 2, width // 8 * 6 // LANE * LANE
    cuts = (wide, wide, wide, even)
    sems = pltpu.SemaphoreType.DMA
    array = lambda *shape: VMEM(shape, jnp.bfloat16)
    any_space, vmem = (pl.BlockSpec(memory_space=space) for space in (pl.ANY, pltpu.VMEM))
    block_weights = [
        array(width, 2 * shares.slot), array(width, 2 * shares.slot), array(2 * shares.slot, width),
        sems((kinds, 8)), sems((kinds, 8)), sems((kinds, 8)), sems((kinds, 8)), sems((kinds,)),
    ]
    return pl.pallas_call(
        functools.partial(layer_kernel, shares, cuts),
        out_shape=jax.ShapeDtypeStruct(stream.shape, jnp.bfloat16),
        in_specs=[any_space, vmem] + [any_space] * 5 + [vmem] * 4 + [any_space] * 4,
        out_specs=any_space,
        scratch_shapes=[
            array(half, width), array(half, width), array(half, width), array(2 * half, width),
            array(2 * half, channels), array(2 * half, width), array(half, width),
            array(half, width), array(width, channels), array(width, channels),
            array(parts, *proj_out.shape),
            array(8 * half, width), array(8 * half, width), array(2 * half, width),
            array(2 * half, width), array(2 * half, width), array(half, width),
            array(half, width),
            sems((4,)), sems((4,)), sems((1,)), sems((3, 14)), sems((3, 14)), sems((3,)),
            sems((2, 9)), sems((2, 9)), sems((2, 3, 6)), sems((2, 3, 6)),
        ] + block_weights + block_weights,
        compiler_params=pltpu.CompilerParams(
            collective_id=1, has_side_effects=True, vmem_limit_bytes=63 * 2**20
        ),
        cost_estimate=pl.CostEstimate(
            flops=12 * stream.shape[0] * gate.shape[1] * width,
            bytes_accessed=64 * gate.shape[1] * width,
            transcendentals=0,
        ),
    )(*args)


def cubes(stream, gate_weight):
    sizes = tuple(lax.axis_size(name) for name in ("rep", "fs", "tp"))
    rows, units = gate_weight.shape
    width = stream.shape[1] * 2
    return (
        sizes == (2, 8, 2)
        and stream.shape[0] % (2 * BLOCK) == 0
        and stream.shape[1] % (2 * LANE) == 0
        and units % (2 * LANE) == 0
        and units >= 16 * LANE
        and rows % 32 == 0
        and width * (12 * units // 8 + 34 * stream.shape[0] // 2 + 6 * 512) * 2 < 60 * 2**20
    )


def feed_forward(stream, gain, gate_weight, up_weight, down_weight):
    normed = normalized(stream, gain)
    gate, up_part = ffn_inputs(normed, gate_weight, up_weight)
    hidden = (jax.nn.silu(gate) * up_part).astype(jnp.bfloat16)
    terms = jnp.dot(
        hidden,
        lax.all_gather(down_weight, "fs", axis=1, tiled=True),
        preferred_element_type=jnp.float32,
    )
    return lax.psum_scatter(
        terms.astype(jnp.bfloat16), "tp", scatter_dimension=1, tiled=True
    ).astype(jnp.float32)


def body(
    resid,
    norm_gains,
    gate_one,
    up_one,
    down_one,
    proj_u,
    proj_v,
    spatial,
    spatial_bias,
    mix_gain,
    head_gain,
    proj_out,
    gate_two,
    up_two,
    down_two,
):
    if cubes(resid, gate_one):
        return whole_layer(
            resid, norm_gains, gate_one, up_one, down_one, proj_u, proj_v, spatial,
            spatial_bias, mix_gain[None], head_gain[None], proj_out, gate_two, up_two, down_two,
        )
    total = feed_forward(resid, norm_gains[0], gate_one, up_one, down_one)
    first = (resid.astype(jnp.float32) + 0.5 * total).astype(jnp.bfloat16)
    mnormed = normalized(first, norm_gains[1])
    u_part, v_part = mixer_inputs(mnormed, proj_u, proj_v)
    proj_out = lax.all_gather(proj_out, "fs", axis=1, tiled=True)
    rows = u_part.shape[0]
    seqs = rows // BLOCK
    local_heads = spatial.shape[0]
    gated_u = jax.nn.gelu(u_part).reshape(seqs, BLOCK, local_heads, HEAD_DIM)
    gated_v = jax.nn.gelu(v_part).reshape(seqs, BLOCK, local_heads, HEAD_DIM)
    centre = jnp.mean(gated_v, axis=-1, keepdims=True)
    spread = jnp.mean(jnp.square(gated_v - centre), axis=-1, keepdims=True)
    vn = (
        (gated_v - centre) * lax.rsqrt(spread + 1e-05) * mix_gain.reshape(local_heads, HEAD_DIM)
    ).astype(jnp.bfloat16)
    segment = jnp.arange(BLOCK) // SPAN
    causal = segment[:, None] >= segment[None, :]
    masked = jnp.where(causal[None], spatial, jnp.zeros_like(spatial))
    mixed = (
        jnp.einsum("hts,bshd->bthd", masked, vn, preferred_element_type=jnp.float32)
        + spatial_bias.T[None, :, :, None]
    )
    product = gated_u * mixed
    gated = (
        rms_scale(product, head_gain.reshape(local_heads, HEAD_DIM))
        .astype(jnp.bfloat16)
        .reshape(rows, local_heads * HEAD_DIM)
    )
    terms = jnp.dot(
        gated,
        proj_out,
        preferred_element_type=jnp.float32,
    )
    branch = lax.psum_scatter(
        terms.astype(jnp.bfloat16), "tp", scatter_dimension=1, tiled=True
    ).astype(jnp.float32)
    second = (first.astype(jnp.float32) + branch).astype(jnp.bfloat16)
    total = feed_forward(second, norm_gains[2], gate_two, up_two, down_two)
    return (second.astype(jnp.float32) + 0.5 * total).astype(jnp.bfloat16)


def solution(mesh):
    return jax.shard_map(
        body,
        mesh=mesh,
        in_specs=(
            P(("rep", "fs"), "tp"),
            P(),
            P("fs", "tp"),
            P("fs", "tp"),
            P("tp", "fs"),
            P("fs", "tp"),
            P("fs", "tp"),
            P("tp", None, None),
            P("tp", None),
            P("tp"),
            P("tp"),
            P("tp", "fs"),
            P("fs", "tp"),
            P("fs", "tp"),
            P("tp", "fs"),
        ),
        out_specs=P(("rep", "fs"), "tp"),
        check_vma=False,
    )
```

```python
import functools

import jax
import jax.numpy as jnp
from jax import lax
from jax.experimental import pallas as pl
from jax.experimental.pallas import tpu as pltpu
from jax.sharding import PartitionSpec as P

HEAD_DIM = 128
BLOCK = 128
SPAN = 64


def rms_scale(values, gain):
    return values * lax.rsqrt(jnp.mean(values * values, axis=-1, keepdims=True) + 1e-06) * gain


def normalized(stream, gain):
    whole = lax.all_gather(stream, "tp", axis=1, tiled=True).astype(jnp.float32)
    return rms_scale(whole, gain).astype(jnp.bfloat16)


def accumulate(left, piece):
    return jnp.dot(left, piece, preferred_element_type=jnp.float32)


def folders(normed):

    def single(total, piece, start):
        return accumulate(normed, piece)

    def double(totals, pieces, start):
        return (accumulate(normed, pieces[0]), accumulate(normed, pieces[1]))

    return (single, double)


def ffn_inputs(normed, first_weight, second_weight):
    empty = jnp.zeros((normed.shape[0], first_weight.shape[1]), jnp.float32)
    single, _ = folders(normed)
    result = (
        single(empty, lax.all_gather(first_weight, "fs", axis=0, tiled=True), jnp.int32(0)),
        single(empty, lax.all_gather(second_weight, "fs", axis=0, tiled=True), jnp.int32(0)),
    )
    return result


def mixer_inputs(normed, first_weight, second_weight):
    empty = jnp.zeros((normed.shape[0], first_weight.shape[1]), jnp.float32)
    single, _ = folders(normed)
    result = (
        single(empty, lax.all_gather(first_weight, "fs", axis=0, tiled=True), jnp.int32(0)),
        single(empty, lax.all_gather(second_weight, "fs", axis=0, tiled=True), jnp.int32(0)),
    )
    return result


LANE = 128
MESH = pl.DeviceIdType.MESH
VMEM = pltpu.VMEM


def flip(value, bit):
    return value + bit - 2 * bit * lax.rem(lax.div(value, jnp.int32(bit)), 2)


def xor(value, mask):
    for bit in (1, 2, 4):
        if mask & bit:
            value = flip(value, bit)
    return value


class Place:
    def __init__(self):
        self.rep, self.fs, self.tp = (lax.axis_index(name) for name in ("rep", "fs", "tp"))
        self.y = lax.rem(self.fs, 2)
        self.z = lax.rem(lax.div(self.fs, jnp.int32(2)), 2)
        self.x_peer = {"rep": 1 - self.rep}
        self.y_peer = {"fs": flip(self.fs, 1)}
        self.z_peer = {"fs": flip(self.fs, 2)}
        self.sibling = {"tp": 1 - self.tp}

    def member(self, mask):
        return xor(4 * self.rep + 2 * self.y + self.z, mask)

    def barrier(self):
        semaphore = pltpu.get_barrier_semaphore()
        peers = [{"fs": xor(self.fs, mask)} for mask in range(1, 8)]
        peers += [self.x_peer, self.sibling]
        for peer in peers:
            pl.semaphore_signal(semaphore, inc=1, device_id=peer, device_id_type=MESH)
        pl.semaphore_wait(semaphore, len(peers))


def remote(src, dst, send, recv, peer):
    return pltpu.make_async_remote_copy(
        src_ref=src, dst_ref=dst, send_sem=send, recv_sem=recv,
        device_id=peer, device_id_type=MESH,
    )


def rows_at(index, size):
    return pl.ds(pl.multiple_of(index * size, size), size)


class Shares:
    def __init__(self, units):
        self.tiles = units // LANE // 2
        self.most = -(-self.tiles // 4)
        self.missing = 4 * self.most - self.tiles
        self.base = (self.most - (1 if self.missing else 0)) * LANE
        self.extra = LANE if self.missing else 0
        self.slot = self.most * LANE

    def of(self, place, quarter, core):
        late = 4 - self.missing
        before = jnp.where(
            core == 0, jnp.maximum(quarter - late, 0), jnp.minimum(quarter, self.missing)
        )
        long = jnp.where(core == 0, quarter < late, quarter >= self.missing)
        start = place.rep * self.tiles + quarter * self.most - before
        return start * LANE, long


class Weights:
    def __init__(self, place, shares, shards, whole, sems):
        self.place, self.shares, self.shards, self.whole = place, shares, shards, whole
        self.send_sem, self.recv_sem, self.pass_send, self.pass_recv, self.local = sems
        self.kinds = 6 if shares.extra else 3
        self.quarter = lax.rem(place.fs, 4)

    def source(self, kind, start):
        shares, which = self.shares, kind % 3
        first = start + (shares.base if kind >= 3 else 0)
        size = shares.extra if kind >= 3 else shares.base
        ref = self.shards[which]
        first = jnp.minimum(first, ref.shape[0 if which == 2 else 1] - size)
        cut = pl.ds(pl.multiple_of(first, LANE), size)
        return ref.at[cut, :] if which == 2 else ref.at[:, cut]

    def target(self, kind, owner, core):
        shares, which = self.shares, kind % 3
        first = core * shares.slot + (shares.base if kind >= 3 else 0)
        size = shares.extra if kind >= 3 else shares.base
        cut = pl.ds(pl.multiple_of(first, LANE), size)
        ref = self.whole[which]
        if which == 2:
            return ref.at[cut, rows_at(owner, self.shards[2].shape[1])]
        return ref.at[rows_at(owner, self.shards[which].shape[0]), cut]

    def when(self, kind, long, action):
        if kind >= 3:
            pl.when(long)(action)
        else:
            action()

    def sent(self, kind, mask):
        return kind if kind < 3 else 3 + 7 * (kind - 3) + mask - 1

    def out(self, kind, mask):
        peer = xor(self.place.fs, mask)
        start, long = self.shares.of(self.place, lax.rem(peer, 4), self.place.tp)
        return long, remote(
            self.source(kind, start),
            self.target(kind, self.place.fs, self.place.tp),
            self.send_sem.at[self.sent(kind, mask)],
            self.recv_sem.at[kind, mask],
            {"fs": peer},
        )

    def start(self, pieces):
        for kind, mask in pieces:
            long, copy = self.out(kind, mask)
            self.when(kind, long, copy.start)

    def own(self):
        start, long = self.shares.of(self.place, self.quarter, self.place.tp)
        for kind in range(self.kinds):
            source = self.source(kind, start)
            target = self.target(kind, self.place.fs, self.place.tp)
            here = pltpu.make_async_copy(source, target, self.local.at[kind])
            there = self.passed(kind, 0, source)

            def begin(here=here, there=there):
                here.start()
                there.start()

            self.when(kind, long, begin)

    def passed(self, kind, mask, source=None):
        target = self.target(kind, xor(self.place.fs, mask), self.place.tp)
        return remote(
            target if source is None else source,
            target,
            self.pass_send.at[kind],
            self.pass_recv.at[kind],
            self.place.sibling,
        )

    def band(self, kind, core, owners):
        shares, which = self.shares, kind % 3
        first = core * shares.slot + (shares.base if kind >= 3 else 0)
        size = shares.extra if kind >= 3 else shares.base
        cut = pl.ds(pl.multiple_of(first, LANE), size)
        ref = self.whole[which]
        if which == 2:
            band = ref.at[cut, pl.ds(0, owners * self.shards[2].shape[1])]
        else:
            band = ref.at[pl.ds(0, owners * self.shards[which].shape[0]), cut]
        return band

    def blank(self):
        shares = self.shares
        if not shares.extra:
            return
        for core in range(2):
            _, long = shares.of(self.place, self.quarter, core)
            cut = pl.ds(core * shares.slot + shares.base, shares.extra)

            def clear(cut=cut):
                for ref in self.whole[:2]:
                    ref[:, cut] = jnp.zeros((ref.shape[0], shares.extra), ref.dtype)
                down = self.whole[2]
                down[cut, :] = jnp.zeros((shares.extra, down.shape[1]), down.dtype)

            pl.when(jnp.logical_not(long))(clear)

    def forward(self, pieces):
        _, long = self.shares.of(self.place, self.quarter, self.place.tp)
        for kind, mask in pieces:
            def step(kind=kind, mask=mask):
                self.out(kind, mask)[1].wait_recv()
                self.passed(kind, mask).start()

            self.when(kind, long, step)

    def finish(self):
        _, long = self.shares.of(self.place, self.quarter, self.place.tp)
        _, other = self.shares.of(self.place, self.quarter, 1 - self.place.tp)
        start, _ = self.shares.of(self.place, self.quarter, self.place.tp)
        for kind in range(self.kinds):
            here = pltpu.make_async_copy(
                self.source(kind, start),
                self.target(kind, self.place.fs, self.place.tp),
                self.local.at[kind],
            )
            self.when(kind, long, here.wait)
            band = self.band(kind, 1 - self.place.tp, 8)
            passed = remote(
                band, band, self.pass_send.at[kind], self.pass_recv.at[kind], self.place.sibling
            )
            self.when(kind, other, passed.wait_recv)

    def drain(self):
        _, long = self.shares.of(self.place, self.quarter, self.place.tp)
        for kind in range(self.kinds):
            if kind >= 3:
                for mask in range(1, 8):
                    sent, copy = self.out(kind, mask)
                    self.when(kind, sent, copy.wait_send)
            else:
                band = self.band(kind, self.place.tp, 7)
                remote(
                    band, band, self.send_sem.at[kind], self.recv_sem.at[kind, 1],
                    self.place.sibling,
                ).wait_send()
            band = self.band(kind, self.place.tp, 8)
            passed = remote(
                band, band, self.pass_send.at[kind], self.pass_recv.at[kind], self.place.sibling
            )
            self.when(kind, long, passed.wait_send)


class Gather:
    def __init__(self, place, tokens, cut, send, recv):
        self.place, self.tokens, self.cut = place, tokens, cut
        self.send, self.recv = send, recv
        self.half = tokens.shape[0] // 8

    def copy(self, index):
        place, width = self.place, self.tokens.shape[1]
        left, right = pl.ds(0, self.cut), pl.ds(self.cut, width - self.cut)
        mask, columns, peer = (
            (0, pl.ds(0, width), place.z_peer),
            (0, pl.ds(0, width), place.y_peer),
            (1, pl.ds(0, width), place.y_peer),
            (0, pl.ds(0, width), place.x_peer),
            (1, pl.ds(0, width), place.x_peer),
            (2, left, place.x_peer),
            (3, left, place.x_peer),
            (4, right, place.y_peer),
            (5, right, place.y_peer),
        )[index]
        block = self.tokens.at[rows_at(place.member(mask), self.half), columns]
        return remote(block, block, self.send.at[index], self.recv.at[index], peer)

    def arrival(self, index):
        place, width = self.place, self.tokens.shape[1]
        left, right = pl.ds(0, self.cut), pl.ds(self.cut, width - self.cut)
        mask, columns = (
            (1, pl.ds(0, width)),
            (2, pl.ds(0, width)),
            (3, pl.ds(0, width)),
            (4, pl.ds(0, width)),
            (5, pl.ds(0, width)),
            (6, left),
            (7, left),
            (6, right),
            (7, right),
        )[index]
        block = self.tokens.at[rows_at(place.member(mask), self.half), columns]
        remote(block, block, self.send.at[index], self.recv.at[index], place.x_peer).wait_recv()

    def drain(self):
        for index in range(9):
            self.copy(index).wait_send()


class Scatter:
    def __init__(self, place, part, cut, relay, from_x, from_y, send_z, from_z, send, recv):
        self.place, self.part, self.cut = place, part, cut
        self.relay, self.from_x, self.from_y = relay, from_x, from_y
        self.send_z, self.from_z = send_z, from_z
        self.send, self.recv = send, recv
        self.half = part.shape[0] // 8
        width = part.shape[1]
        self.left, self.right = pl.ds(0, cut), pl.ds(cut, width - cut)

    def block(self, turn, mask):
        return rows_at(self.place.member(2 * mask + 1 - turn), self.half)

    def copy(self, turn, index):
        place = self.place
        mask, columns, target, peer = (
            (3, self.left, self.relay, place.x_peer),
            (3, self.right, self.relay, place.y_peer),
            (2, self.left, self.from_x, place.x_peer),
            (1, self.right, self.from_y, place.y_peer),
            (1, self.left, self.from_y, place.y_peer),
            (2, self.right, self.from_x, place.x_peer),
        )[index]
        return remote(
            self.part.at[self.block(turn, mask), columns],
            target.at[pl.ds(turn * self.half, self.half), columns],
            self.send.at[6 * turn + index],
            self.recv.at[6 * turn + index],
            peer,
        )

    def add(self, turn, index):
        columns, mask = ((self.left, 1), (self.right, 2))[index]
        self.copy(turn, index).wait_recv()
        rows = self.block(turn, mask)
        got = self.relay[pl.ds(turn * self.half, self.half), columns]
        mine = self.part[rows, columns]
        total = mine.astype(jnp.float32) + got.astype(jnp.float32)
        self.part[rows, columns] = total.astype(self.part.dtype)
        self.copy(turn, 4 + index).start()

    def total(self, turn):
        for index in range(2, 6):
            self.copy(turn, index).wait_recv()
        rows = pl.ds(turn * self.half, self.half)
        result = self.part[self.block(turn, 0), :].astype(jnp.float32)
        result = result + self.from_x[rows, :].astype(jnp.float32)
        return result + self.from_y[rows, :].astype(jnp.float32)

    def z_copy(self):
        return remote(
            self.send_z, self.from_z, self.send.at[12], self.recv.at[12], self.place.z_peer
        )

    def drain(self):
        for turn in range(2):
            for index in range(6):
                self.copy(turn, index).wait_send()
        self.z_copy().wait_send()


def product(left, right):
    return jnp.dot(left, right, preferred_element_type=jnp.float32)


def gather_start(gather):
    for index in (0, 1, 3):
        gather.copy(index).start()


def gather_near(gather):
    gather.arrival(0)
    gather.copy(2).start()
    gather.copy(4).start()


def gather_relay(gather):
    for index, relays in ((1, 5), (3, 7), (2, 6), (4, 8)):
        gather.arrival(index)
        gather.copy(relays).start()


def gather_finish(gather):
    for index in range(5, 9):
        gather.arrival(index)


def block_sums(place, gather, weights, scatter, soon, later, last):
    gate, up, down = weights.whole
    size = 2 * gather.half

    def quadrant(step, carry):
        @pl.when(step == 3)
        def relay():
            scatter.add(0, 0)
            scatter.add(0, 1)
            for index in (0, 2, 3):
                scatter.copy(1, index).start()

        mask = 3 - step
        rep = lax.rem(place.rep + lax.div(mask, jnp.int32(2)), 2)
        y = lax.rem(place.y + lax.rem(mask, 2), 2)
        rows = rows_at(2 * rep + y, size)
        tokens = gather.tokens[rows, :]
        hidden = (
            jax.nn.silu(product(tokens, gate[...])) * product(tokens, up[...])
        ).astype(jnp.bfloat16)
        scatter.part[rows, :] = product(hidden, down[...]).astype(jnp.bfloat16)

        for which, copies in ((0, ((0, 0), (0, 1), (1, 1))), (1, ((0, 2),)), (2, ((0, 3),))):
            def send(copies=copies):
                for turn, index in copies:
                    scatter.copy(turn, index).start()

            pl.when(step == which)(send)
        return carry

    lax.fori_loop(0, 4, quadrant, jnp.int32(0))
    gather.drain()
    soon()
    scatter.send_z[...] = scatter.total(0).astype(jnp.bfloat16)
    scatter.z_copy().start()
    scatter.add(1, 0)
    scatter.add(1, 1)
    later()
    last()
    result = scatter.total(1)
    scatter.z_copy().wait_recv()
    return result + scatter.from_z[...].astype(jnp.float32)


class Mixing:
    SLOTS = tuple(
        [("far", 0)]
        + [("z", mask) for mask in (0, 4)]
        + [("y", mask) for mask in (0, 4, 2, 6)]
        + [("x", mask) for mask in (4, 2, 6, 1, 5, 3, 7)]
    )

    def __init__(self, place, shards, whole, send, recv, local):
        self.place, self.shards, self.whole = place, shards, whole
        self.send, self.recv, self.local = send, recv, local

    def part(self, kind, half):
        size = self.shards[kind].shape[0] // 2
        return self.shards[kind].at[rows_at(half, size), :]

    def target(self, kind, owner, half):
        size = self.shards[kind].shape[0] // 2
        if kind == 2:
            return self.whole[2].at[owner, rows_at(half, size), :]
        return self.whole[kind].at[rows_at(2 * owner + half, size), :]

    def copy(self, kind, slot):
        place = self.place
        way, mask = self.SLOTS[slot]
        peer = {
            "far": {"fs": xor(place.fs, 4)},
            "y": place.y_peer,
            "z": place.z_peer,
            "x": place.x_peer,
        }[way]
        target = self.target(kind, xor(place.fs, mask), place.rep)
        source = target if mask else self.part(kind, place.rep)
        return remote(source, target, self.send.at[kind], self.recv.at[kind, slot], peer)

    def start(self, slots):
        for slot in slots:
            for kind in range(3):
                self.copy(kind, slot).start()

    def arrive(self, slots):
        place = self.place
        for slot in slots:
            way, mask = self.SLOTS[slot]
            mask ^= {"far": 4, "y": 1, "z": 2, "x": 0}[way]
            half = 1 - place.rep if way == "x" else place.rep
            for kind in range(3):
                target = self.target(kind, xor(place.fs, mask), half)
                remote(
                    target, target, self.send.at[kind], self.recv.at[kind, slot],
                    place.x_peer,
                ).wait_recv()

    def own(self):
        copies = []
        for kind in range(3):
            size = self.shards[kind].shape[0]
            target = (
                self.whole[2].at[self.place.fs]
                if kind == 2
                else self.whole[kind].at[rows_at(self.place.fs, size), :]
            )
            copies.append(
                pltpu.make_async_copy(self.shards[kind], target, self.local.at[kind])
            )
        return copies

    def drain(self):
        halves = len(self.SLOTS)
        for kind in range(3):
            if kind == 2:
                band = self.whole[2].at[pl.ds(0, halves // 2)]
            else:
                band = self.whole[kind].at[pl.ds(0, halves // 2 * self.shards[kind].shape[0]), :]
            remote(
                band, band, self.send.at[kind], self.recv.at[kind, 0], self.place.x_peer
            ).wait_send()


def mix(place, first, normed_rows, projections, mixing, gated, terms, other, send, recv):
    spatial, bias, mix_gain, head_gain = mixing
    pu, pv, po = projections
    half = first.shape[0]
    own, sibling = rows_at(place.tp, half), rows_at(1 - place.tp, half)
    remote(
        normed_rows.at[sibling, :], normed_rows.at[sibling, :], send.at[1], recv.at[1],
        place.sibling,
    ).wait_recv()
    row = lax.broadcasted_iota(jnp.int32, (BLOCK, BLOCK), 0)
    column = lax.broadcasted_iota(jnp.int32, (BLOCK, BLOCK), 1)
    causal = lax.div(row, SPAN) >= lax.div(column, SPAN)
    u_part = jax.nn.gelu(product(normed_rows[...], pu[...]))
    v_part = jax.nn.gelu(product(normed_rows[...], pv[...]))
    for head in range(spatial.shape[0]):
        at = slice(head * HEAD_DIM, (head + 1) * HEAD_DIM)
        matrix = jnp.where(causal, spatial[head], jnp.zeros_like(spatial[head]))
        shift = jnp.sum(
            jnp.where(row == column, bias[head : head + 1, :], 0.0), axis=1, keepdims=True
        )
        for start in range(0, 2 * half, BLOCK):
            rows = slice(start, start + BLOCK)
            value = v_part[rows, at]
            centred = value - jnp.mean(value, axis=-1, keepdims=True)
            spread = jnp.mean(jnp.square(centred), axis=-1, keepdims=True)
            vn = (centred * lax.rsqrt(spread + 1e-05) * mix_gain[:, at]).astype(jnp.bfloat16)
            mixed = product(matrix, vn) + shift
            gated[rows, at] = rms_scale(u_part[rows, at] * mixed, head_gain[:, at]).astype(
                jnp.bfloat16
            )
    for part in range(po.shape[0]):
        at = pl.ds(part * po.shape[2], po.shape[2])
        terms[:, at] = product(gated[...], po[part]).astype(jnp.bfloat16)
    swap = remote(terms.at[sibling, :], other, send.at[2], recv.at[2], place.sibling)
    swap.start()
    swap.wait_recv()
    branch = terms[own, :].astype(jnp.float32) + other[...].astype(jnp.float32)
    return first[...].astype(jnp.float32) + branch


def near_pieces(kinds):
    return [(kind, mask) for kind in kinds for mask in (1, 2, 3)]


def far_pieces(kinds):
    return [(kind, mask) for kind in kinds for mask in (4, 5, 6, 7)]


def layer_kernel(shares, cuts, *refs):
    (stream, gains, gate_one, up_one, down_one, proj_u, proj_v, spatial, bias, mix_gain,
     head_gain, proj_out, gate_two, up_two, down_two, out) = refs[:16]
    (mine, first, second, normed_rows, gated, terms, other, result, pu, pv, po,
     tokens, part, relay, from_x, from_y, send_z, from_z) = refs[16:34]
    send, recv, local, mix_send, mix_recv, mix_local = refs[34:40]
    ag_send, ag_recv, rs_send, rs_recv = refs[40:44]
    place = Place()
    weights, gathers, scatters = [], [], []
    for which, shards in enumerate(((gate_one, up_one, down_one), (gate_two, up_two, down_two))):
        whole, sems = refs[44 + 8 * which : 47 + 8 * which], refs[47 + 8 * which : 52 + 8 * which]
        weights.append(Weights(place, shares, shards, whole, sems))
        gathers.append(Gather(place, tokens, cuts[2 * which], ag_send.at[which], ag_recv.at[which]))
        scatters.append(
            Scatter(place, part, cuts[2 * which + 1], relay, from_x, from_y, send_z, from_z,
                    rs_send.at[which], rs_recv.at[which])
        )
    mixing = Mixing(place, (proj_u, proj_v, proj_out), (pu, pv, po), mix_send, mix_recv, mix_local)
    half, _ = mine.shape
    share = stream.shape[1]
    place.barrier()

    own, sibling = rows_at(place.tp, half), rows_at(1 - place.tp, half)
    columns = rows_at(place.tp, share)
    there = remote(
        stream.at[sibling, :], mine.at[:, columns], send.at[0], recv.at[0], place.sibling
    )
    here = pltpu.make_async_copy(stream.at[own, :], mine.at[:, columns], local.at[0])
    there.start()
    here.start()
    mixing.start((0, 1, 3))
    one, two = weights
    for copy in mixing.own():
        copy.start()
    here.wait()
    there.wait_recv()
    block = rows_at(place.member(0), half)
    normed = rms_scale(mine[...].astype(jnp.float32), gains[0:1, :])
    tokens[block, :] = normed.astype(jnp.bfloat16)
    gather_start(gathers[0])
    extras = (3, 4, 5) if shares.extra else ()
    one.start(far_pieces((0,)))
    one.own()
    one.blank()
    two.blank()
    mixing.arrive((0,))
    mixing.start((2, 4, 7))
    one.start(far_pieces((1,)))
    mixing.arrive((1, 3))
    mixing.start((5, 8, 10))
    gather_near(gathers[0])
    mixing.arrive((2, 4))
    mixing.start((6, 9, 11))
    one.start(far_pieces((2,) + extras))
    one.start(near_pieces((0, 1, 2) + extras))
    gather_relay(gathers[0])
    mixing.arrive((5, 6))
    mixing.start((12, 13))
    one.forward(far_pieces((0, 1, 2) + extras) + near_pieces((0, 1, 2) + extras))
    gather_finish(gathers[0])
    two.start(far_pieces((0,)))
    one.finish()
    total = block_sums(
        place, gathers[0], one, scatters[0],
        lambda: two.start(far_pieces((1,))),
        lambda: two.start([(kind, mask) for kind in (0, 1) for mask in (1, 3)]),
        lambda: two.start(far_pieces((2,))),
    )
    first[...] = (mine[...].astype(jnp.float32) + 0.5 * total).astype(jnp.bfloat16)

    normed = rms_scale(first[...].astype(jnp.float32), gains[1:2, :])
    normed_rows[own, :] = normed.astype(jnp.bfloat16)
    trade = remote(
        normed_rows.at[own, :], normed_rows.at[own, :], send.at[1], recv.at[1], place.sibling
    )
    trade.start()
    two.own()
    for copy in mixing.own():
        copy.wait()
    mixing.arrive(range(7, 14))
    second[...] = mix(
        place, first, normed_rows, (pu, pv, po), (spatial, bias, mix_gain, head_gain),
        gated, terms, other, send, recv,
    ).astype(jnp.bfloat16)
    scatters[0].drain()
    normed = rms_scale(second[...].astype(jnp.float32), gains[2:3, :])
    tokens[block, :] = normed.astype(jnp.bfloat16)
    gather_start(gathers[1])
    one.drain()
    mixing.drain()
    gather_near(gathers[1])
    two.start(far_pieces(extras) + near_pieces(extras) + [(2, 1), (2, 3), (0, 2), (1, 2), (2, 2)])
    gather_relay(gathers[1])
    two.forward(far_pieces((0, 1, 2) + extras) + near_pieces((0, 1, 2) + extras))
    gather_finish(gathers[1])
    two.finish()
    total = block_sums(place, gathers[1], two, scatters[1], lambda: None, lambda: None, two.drain)
    result[...] = (second[...].astype(jnp.float32) + 0.5 * total).astype(jnp.bfloat16)

    last = remote(
        result.at[:, rows_at(1 - place.tp, share)], out.at[own, :],
        send.at[3], recv.at[3], place.sibling,
    )
    last.start()
    keep = pltpu.make_async_copy(
        result.at[:, rows_at(place.tp, share)], out.at[own, :], local.at[0]
    )
    keep.start()
    there.wait_send()
    trade.wait_send()
    remote(terms.at[sibling, :], other, send.at[2], recv.at[2], place.sibling).wait_send()
    scatters[1].drain()
    last.wait_send()
    keep.wait()
    remote(
        result.at[:, rows_at(1 - place.tp, share)], out.at[sibling, :],
        send.at[3], recv.at[3], place.sibling,
    ).wait_recv()


def whole_layer(*args):
    stream, gate, proj_u, proj_out = args[0], args[2], args[5], args[11]
    half, width = stream.shape[0] // 2, 2 * stream.shape[1]
    shares = Shares(gate.shape[1])
    channels = proj_u.shape[1]
    kinds = 6 if shares.extra else 3
    parts = lax.axis_size("fs")
    even, wide = width // 2, width // 8 * 6 // LANE * LANE
    broad = width // 8 * 7 // LANE * LANE
    cuts = (broad, wide, broad, even)
    sems = pltpu.SemaphoreType.DMA
    array = lambda *shape: VMEM(shape, jnp.bfloat16)
    any_space, vmem = (pl.BlockSpec(memory_space=space) for space in (pl.ANY, pltpu.VMEM))
    block_weights = [
        array(width, 2 * shares.slot), array(width, 2 * shares.slot), array(2 * shares.slot, width),
        sems((3 + 7 * (kinds - 3),)), sems((kinds, 8)), sems((kinds,)), sems((kinds,)),
        sems((kinds,)),
    ]
    return pl.pallas_call(
        functools.partial(layer_kernel, shares, cuts),
        out_shape=jax.ShapeDtypeStruct(stream.shape, jnp.bfloat16),
        in_specs=[any_space, vmem] + [any_space] * 5 + [vmem] * 4 + [any_space] * 4,
        out_specs=any_space,
        scratch_shapes=[
            array(half, width), array(half, width), array(half, width), array(2 * half, width),
            array(2 * half, channels), array(2 * half, width), array(half, width),
            array(half, width), array(width, channels), array(width, channels),
            array(parts, *proj_out.shape),
            array(8 * half, width), array(8 * half, width), array(2 * half, width),
            array(2 * half, width), array(2 * half, width), array(half, width),
            array(half, width),
            sems((4,)), sems((4,)), sems((1,)), sems((3,)), sems((3, 14)), sems((3,)),
            sems((2, 9)), sems((2, 9)), sems((2, 13)), sems((2, 13)),
        ] + block_weights + block_weights,
        compiler_params=pltpu.CompilerParams(
            collective_id=1, has_side_effects=True, vmem_limit_bytes=63 * 2**20
        ),
        cost_estimate=pl.CostEstimate(
            flops=12 * stream.shape[0] * gate.shape[1] * width,
            bytes_accessed=64 * gate.shape[1] * width,
            transcendentals=0,
        ),
    )(*args)


def cubes(stream, gate_weight):
    sizes = tuple(lax.axis_size(name) for name in ("rep", "fs", "tp"))
    rows, units = gate_weight.shape
    width = stream.shape[1] * 2
    return (
        sizes == (2, 8, 2)
        and stream.shape[0] % (2 * BLOCK) == 0
        and stream.shape[1] % (2 * LANE) == 0
        and units % (2 * LANE) == 0
        and units >= 16 * LANE
        and rows % 32 == 0
        and width * (12 * units // 8 + 34 * stream.shape[0] // 2 + 6 * 512) * 2 < 60 * 2**20
    )


def feed_forward(stream, gain, gate_weight, up_weight, down_weight):
    normed = normalized(stream, gain)
    gate, up_part = ffn_inputs(normed, gate_weight, up_weight)
    hidden = (jax.nn.silu(gate) * up_part).astype(jnp.bfloat16)
    terms = jnp.dot(
        hidden,
        lax.all_gather(down_weight, "fs", axis=1, tiled=True),
        preferred_element_type=jnp.float32,
    )
    return lax.psum_scatter(
        terms.astype(jnp.bfloat16), "tp", scatter_dimension=1, tiled=True
    ).astype(jnp.float32)


def body(
    resid,
    norm_gains,
    gate_one,
    up_one,
    down_one,
    proj_u,
    proj_v,
    spatial,
    spatial_bias,
    mix_gain,
    head_gain,
    proj_out,
    gate_two,
    up_two,
    down_two,
):
    if cubes(resid, gate_one):
        return whole_layer(
            resid, norm_gains, gate_one, up_one, down_one, proj_u, proj_v, spatial,
            spatial_bias, mix_gain[None], head_gain[None], proj_out, gate_two, up_two, down_two,
        )
    total = feed_forward(resid, norm_gains[0], gate_one, up_one, down_one)
    first = (resid.astype(jnp.float32) + 0.5 * total).astype(jnp.bfloat16)
    mnormed = normalized(first, norm_gains[1])
    u_part, v_part = mixer_inputs(mnormed, proj_u, proj_v)
    proj_out = lax.all_gather(proj_out, "fs", axis=1, tiled=True)
    rows = u_part.shape[0]
    seqs = rows // BLOCK
    local_heads = spatial.shape[0]
    gated_u = jax.nn.gelu(u_part).reshape(seqs, BLOCK, local_heads, HEAD_DIM)
    gated_v = jax.nn.gelu(v_part).reshape(seqs, BLOCK, local_heads, HEAD_DIM)
    centre = jnp.mean(gated_v, axis=-1, keepdims=True)
    spread = jnp.mean(jnp.square(gated_v - centre), axis=-1, keepdims=True)
    vn = (
        (gated_v - centre) * lax.rsqrt(spread + 1e-05) * mix_gain.reshape(local_heads, HEAD_DIM)
    ).astype(jnp.bfloat16)
    segment = jnp.arange(BLOCK) // SPAN
    causal = segment[:, None] >= segment[None, :]
    masked = jnp.where(causal[None], spatial, jnp.zeros_like(spatial))
    mixed = (
        jnp.einsum("hts,bshd->bthd", masked, vn, preferred_element_type=jnp.float32)
        + spatial_bias.T[None, :, :, None]
    )
    product = gated_u * mixed
    gated = (
        rms_scale(product, head_gain.reshape(local_heads, HEAD_DIM))
        .astype(jnp.bfloat16)
        .reshape(rows, local_heads * HEAD_DIM)
    )
    terms = jnp.dot(
        gated,
        proj_out,
        preferred_element_type=jnp.float32,
    )
    branch = lax.psum_scatter(
        terms.astype(jnp.bfloat16), "tp", scatter_dimension=1, tiled=True
    ).astype(jnp.float32)
    second = (first.astype(jnp.float32) + branch).astype(jnp.bfloat16)
    total = feed_forward(second, norm_gains[2], gate_two, up_two, down_two)
    return (second.astype(jnp.float32) + 0.5 * total).astype(jnp.bfloat16)


def solution(mesh):
    return jax.shard_map(
        body,
        mesh=mesh,
        in_specs=(
            P(("rep", "fs"), "tp"),
            P(),
            P("fs", "tp"),
            P("fs", "tp"),
            P("tp", "fs"),
            P("fs", "tp"),
            P("fs", "tp"),
            P("tp", None, None),
            P("tp", None),
            P("tp"),
            P("tp"),
            P("tp", "fs"),
            P("fs", "tp"),
            P("fs", "tp"),
            P("tp", "fs"),
        ),
        out_specs=P(("rep", "fs"), "tp"),
        check_vma=False,
    )
```
